128 devices in a mesh: kv: 32 (over z, y, core), tp: 4 (over x).
Axes of the slice: x: 4, y: 4, z: 4, core: 2. Of those that a mesh axis runs over, the one named last changes fastest.
Arguments:
- tokens: bfloat16 [16384, 2048], P('kv', 'tp'), may hold values from -9 to 9
- w_query: bfloat16 [2048, 1536], P(None, 'tp'), may hold values from -1 to 1
- w_key: bfloat16 [2048, 1536], P(None, 'tp'), may hold values from -1 to 1
- w_value: bfloat16 [2048, 1536], P(None, 'tp'), may hold values from -0.5 to 0.5
- w_out: bfloat16 [1536, 2048], P('tp'), may hold values from -0.15625 to 0.15625
- chosen: int32 [512, 24], P('kv'), may hold values from 0 to 511, as said below
Outputs:
- mixed: bfloat16 [16384, 2048], P(('kv', 'tp'))
The draws below stay inside these ranges and needn't reach their ends.
Inputs may be any that keep to these rules, and one draw needn't show every extreme that they name: `chosen`: row c names blocks no later than c; its first entry is c and its second c - 1 (0 for row 0), and an entry may repeat. Taking the rows in aligned runs of 16, one run for each index of kv, the rows of one run name at most 2 distinct blocks lying in any one other index's positions; in every draw some index of kv names exactly 2 from every earlier index. Every run names some block of the index just before it and of the index half the axis before it, where those exist.
All inputs are finite; a program needn't handle non-finite values.
Results may differ from the reference program's by a relative error of at most 0.014.
Values may be sent and summed in bfloat16 or wider, within the bound.
A program may use at most 320 MiB of HBM per device.

```python
import math
import jax
import jax.numpy as jnp
from jax import lax

D = 2048
HEADS = 12
HD = 128
BLK = 32
SEL = 24
MOST = 2
TOK_DEV = 512
TOKENS = 16384
N_KV = 32
N_TP = 4


def draw_tokens(key, part):
    base_key = jax.random.fold_in(key, 7)
    first, second, third = jax.random.split(base_key, 3)
    values = jnp.clip(jax.random.normal(first, (TOKENS, D), jnp.float32), -8.0, 8.0)
    return values.astype(jnp.bfloat16)


def weight_pair(key):
    first = jax.random.normal(jax.random.fold_in(key, 101), (D, HEADS * HD), jnp.float32) / math.sqrt(D)
    second = jax.random.normal(jax.random.fold_in(key, 102), (D, HEADS * HD), jnp.float32) / math.sqrt(D)
    return (first, second)


def draw_w_query(key, part):
    first, second = weight_pair(key)
    return jnp.clip(2.0 * first, -1.0, 1.0).astype(jnp.bfloat16)


def draw_w_key(key, part):
    first, second = weight_pair(key)
    values = second
    return jnp.clip(values, -1.0, 1.0).astype(jnp.bfloat16)


def draw_chosen(key, part):
    per_dev = TOK_DEV // BLK
    ndevs = N_KV
    nblocks = per_dev * ndevs
    keys = jax.random.split(jax.random.fold_in(key, 11), 7)
    popular = jnp.maximum(jax.random.randint(keys[0], (nblocks,), 0, 8) - 4, 0)
    noise = jax.random.randint(keys[1], (nblocks,), 0, 4096)
    block_ids = jnp.arange(nblocks, dtype=jnp.int32)
    score = popular * (1 << 24) + noise * 256 + block_ids % per_dev
    devices = jnp.arange(ndevs, dtype=jnp.int32)
    full_dev = jax.random.randint(keys[2], (), 1, ndevs)
    extra_full = jax.random.randint(keys[3], (ndevs,), 0, 4) == 0
    counts = jax.random.randint(keys[4], (ndevs, ndevs), 0, MOST + 1)
    is_full = (devices == full_dev) | extra_full
    counts = jnp.where(is_full[:, None], MOST, counts)
    before = devices[None, :] == devices[:, None] - 1
    halfway = devices[None, :] == devices[:, None] - ndevs // 2
    counts = jnp.where(before | halfway, jnp.maximum(counts, 1), counts)
    counts = jnp.where(devices[None, :] < devices[:, None], counts, 0)
    boost = (block_ids[None, :] == devices[:, None] * per_dev - 1).astype(jnp.int32) * (1 << 30)
    dev_score = (score[None, :] + boost).reshape(ndevs, ndevs, per_dev)
    ranks = jnp.sum((dev_score[:, :, None, :] > dev_score[:, :, :, None]).astype(jnp.int32), axis=-1)
    in_pool = (ranks < counts[:, :, None]).reshape(ndevs, nblocks)
    pool_pos = jnp.cumsum(in_pool.astype(jnp.int32), axis=1) - 1
    pool_size = jnp.sum(in_pool.astype(jnp.int32), axis=1)
    fill_slots = SEL - 2
    places = jnp.arange(fill_slots * per_dev, dtype=jnp.int32)
    hit = in_pool[:, None, :] & (pool_pos[:, None, :] == places[None, :, None])
    elements = jnp.sum(hit.astype(jnp.int32) * block_ids[None, None, :], axis=-1)
    rows_in = jnp.arange(per_dev, dtype=jnp.int32)
    slot_in = jnp.arange(fill_slots, dtype=jnp.int32)
    place_idx = slot_in[None, :] * per_dev + rows_in[:, None]
    random_pick = jax.random.randint(keys[5], (ndevs, per_dev, fill_slots), 0, 1 << 20)
    safe_size = jnp.maximum(pool_size, 1)[:, None, None]
    take = jnp.where(place_idx[None] < pool_size[:, None, None], place_idx[None], random_pick % safe_size)
    picked = jnp.take_along_axis(elements, take.reshape(ndevs, -1), axis=1).reshape(ndevs, per_dev, fill_slots)
    own_block = devices[:, None] * per_dev + rows_in[None, :]
    own_fill = devices[:, None, None] * per_dev + random_pick % (rows_in[None, :, None] + 1)
    filled = jnp.where(pool_size[:, None, None] > 0, picked, own_fill)
    prev_block = jnp.maximum(own_block - 1, 0)
    rows = jnp.concatenate([own_block[:, :, None], prev_block[:, :, None], filled], axis=-1)
    return rows.reshape(nblocks, SEL).astype(jnp.int32)


def steps_of(rng, dims, cuts, low, top_value):
    def one(axis_at, parts):
        steps = jax.random.uniform(jax.random.fold_in(jax.random.fold_in(rng, 6), axis_at), (parts,), jnp.float32, low / len(cuts), top_value / len(cuts))
        return jnp.repeat(jnp.exp(steps), dims[axis_at] // parts).reshape((-1,) + (1,) * (len(dims) - axis_at - 1))

    gain = one(*cuts[0])
    for cut in cuts[1:]:
        gain = gain * one(*cut)
    return gain


def gaussian(rng, extent, width, limit, cuts=(), kind=jnp.bfloat16):
    gain = steps_of(rng, extent, cuts, -0.22, 0.18) if cuts else 1.0
    values = jax.random.normal(rng, extent, jnp.float32) * width * gain
    return jnp.minimum(jnp.maximum(values, -limit), limit).astype(kind)


def setup_inputs(seed: int = 0) -> dict:
    key_of = jax.random.split(jax.random.key(seed), 7)
    tokens = draw_tokens(jax.random.fold_in(key_of[6], 71), 0)
    w_query = draw_w_query(jax.random.fold_in(key_of[6], 71), 0)
    w_key = draw_w_key(jax.random.fold_in(key_of[6], 71), 0)
    w_value = gaussian(key_of[3], (D, HEADS * HD), (D // 16) ** -0.5, 0.5, ((1, 4),))
    w_out = gaussian(key_of[4], (HEADS * HD, D), (HEADS * HD) ** -0.5, 0.15625, ((0, 4),))
    chosen = draw_chosen(jax.random.fold_in(key_of[6], 71), 0)
    return {"tokens": tokens, "w_query": w_query, "w_key": w_key, "w_value": w_value, "w_out": w_out, "chosen": chosen}


NEG = -1e30


def reference(tokens, w_query, w_key, w_value, w_out, chosen):
    query_rows = jnp.dot(tokens, w_query, preferred_element_type=jnp.float32).astype(jnp.bfloat16)
    key_rows = jnp.dot(tokens, w_key, preferred_element_type=jnp.float32).astype(jnp.bfloat16)
    value_rows = jnp.dot(tokens, w_value, preferred_element_type=jnp.float32).astype(jnp.bfloat16)
    total_rows = tokens.shape[0]
    block_count = total_rows // BLK
    query_blocks = query_rows.reshape(block_count, BLK, HEADS, HD)
    key_blocks = key_rows.reshape(block_count, BLK, HEADS, HD)
    value_blocks = value_rows.reshape(block_count, BLK, HEADS, HD)
    offsets = jnp.arange(BLK, dtype=jnp.int32)
    slot_ids = jnp.arange(SEL, dtype=jnp.int32)
    earlier_slot = slot_ids[None, :] < slot_ids[:, None]

    def one_block(packed):
        query_block, chosen_row, block_index = packed
        repeat_slot = jnp.any((chosen_row[:, None] == chosen_row[None, :]) & earlier_slot, axis=1)
        gathered_keys = key_blocks[chosen_row].astype(jnp.float32)
        gathered_values = value_blocks[chosen_row].astype(jnp.float32)
        scores = jnp.einsum('qhd,jkhd->hqjk', query_block.astype(jnp.float32), gathered_keys) * (HD ** -0.5)
        key_pos = chosen_row[:, None] * BLK + offsets[None, :]
        query_pos = block_index * BLK + offsets
        allowed = (~repeat_slot)[None, :, None] & (key_pos[None, :, :] <= query_pos[:, None, None])
        scores = jnp.where(allowed[None], scores, NEG)
        weights = jax.nn.softmax(scores.reshape(HEADS, BLK, SEL * BLK), axis=-1).reshape(HEADS, BLK, SEL, BLK)
        mixed_heads = jnp.einsum('hqjk,jkhd->qhd', weights, gathered_values)
        return mixed_heads.astype(jnp.bfloat16).reshape(BLK, HEADS * HD)

    attended = lax.map(one_block, (query_blocks, chosen, jnp.arange(block_count, dtype=jnp.int32)))
    attended = attended.reshape(total_rows, HEADS * HD)
    group_width = HEADS * HD // N_TP
    summed = jnp.zeros((total_rows, w_out.shape[1]), jnp.float32)
    for group in range(N_TP):
        partial_value = jnp.dot(attended[:, group * group_width:(group + 1) * group_width],
                          w_out[group * group_width:(group + 1) * group_width],
                          preferred_element_type=jnp.float32).astype(jnp.bfloat16)
        partial_value = lax.optimization_barrier(partial_value)
        summed = summed + partial_value.astype(jnp.float32)
    return summed.astype(jnp.bfloat16)
```

```python
import functools
import math

import jax
import jax.numpy as jnp
from jax import lax
from jax.experimental import pallas as pl
from jax.experimental.pallas import tpu as pltpu
from jax.sharding import Mesh
from jax.sharding import PartitionSpec as P

HD = 128
BLK = 32
SEL = 24
KV = ("kv_0", "kv_1", "kv_2")
KV_TP = ("kv_0", "kv_1", "kv_2", "tp")
NEG = -1e30
MESH = pl.DeviceIdType.MESH
F32 = jnp.float32
BF16 = jnp.bfloat16
CHUNKS = 4
LOG2E = 1.4426950408889634


def dot(a, b):
    return jnp.dot(a, b, preferred_element_type=F32)


def dot_t(a, b):
    return lax.dot_general(a, b, (((1,), (1,)), ((), ())), preferred_element_type=F32)


class Ring:
    def __init__(self, buf, axis, base, rows, coords, sems):
        self.buf, self.axis, self.base, self.rows = buf, axis, base, rows
        self.me = coords[axis]
        self.right = lax.rem(self.me + 1, 4)
        self.left = lax.rem(self.me + 3, 4)
        self.opp = lax.rem(self.me + 2, 4)
        self.coords = coords
        self.send, self.recv = sems
        self.sent = []

    def _copy(self, slot, start, size, target, kind, i):
        view = self.buf.at[slot, pl.ds(self.base + start, size)]
        return pltpu.make_async_remote_copy(
            src_ref=view,
            dst_ref=view,
            send_sem=self.send.at[kind, i],
            recv_sem=self.recv.at[kind, i],
            device_id=tuple(target if a == self.axis else self.coords[a] for a in KV_TP),
            device_id_type=MESH,
        )

    def start_own(self, i):
        for kind, target in ((0, self.right), (1, self.left)):
            copy = self._copy(self.me, i * self.rows, self.rows, target, kind, i)
            copy.start()
            self.sent.append(copy)

    def wait_sides(self, i):
        self._copy(self.left, i * self.rows, self.rows, self.right, 0, i).wait_recv()
        self._copy(self.right, i * self.rows, self.rows, self.left, 1, i).wait_recv()

    def forward(self, i):
        half = self.rows // 2
        for kind, slot, start, target in (
            (2, self.left, i * self.rows, self.right),
            (3, self.right, i * self.rows + half, self.left),
        ):
            copy = self._copy(slot, start, half, target, kind, i)
            copy.start()
            self.sent.append(copy)

    def wait_opp(self, i):
        half = self.rows // 2
        self._copy(self.opp, i * self.rows, half, self.right, 2, i).wait_recv()
        self._copy(self.opp, i * self.rows + half, half, self.left, 3, i).wait_recv()

    def drain(self):
        for copy in self.sent:
            copy.wait_send()


def body(
    tok_hbm, wq_hbm, wk_hbm, wv_hbm, wo_hbm, chosen_ref,
    out_ref,
    x_buf, w_buf, q_buf, k_buf, v_buf, wo_buf,
    stk, stv, fark, farv, att_buf, attx,
    bias_own, bias_far, m_buf, l_buf, acc_buf,
    req_row, req_col, smem_row, smem_col,
    local_sem, req_send, req_recv,
    x_send, x_recv, k_send, k_recv, v_send, v_recv, o_send, o_recv,
    ks_send, ks_recv, vs_send, vs_recv, d_send, d_recv, a_send, a_recv,
):
    z, y, c, t = (lax.axis_index(a) for a in KV_TP)
    coords = dict(zip(KV_TP, (z, y, c, t)))
    me = z * 8 + y * 2 + c
    yc = y * 2 + c
    zc = z * 2 + c

    locals_ = [pltpu.make_async_copy(tok_hbm, x_buf.at[t], local_sem.at[0])]
    for n, w in enumerate((wq_hbm, wk_hbm, wv_hbm)):
        locals_.append(
            pltpu.make_async_copy(w, w_buf.at[:, :, pl.ds(n * 384, 384)], local_sem.at[1 + n])
        )
    locals_.append(pltpu.make_async_copy(wo_hbm, wo_buf.at[t], local_sem.at[4]))
    for copy in locals_:
        copy.start()

    def row_peer(n):
        j = lax.rem(yc + n, 8)
        return j, (z, j // 2, lax.rem(j, 2), t)

    def col_peer(n):
        j = lax.rem(zc + n, 8)
        return j, (j // 2, y, lax.rem(j, 2), t)

    barrier = pltpu.get_barrier_semaphore()
    for n in range(1, 4):
        pl.semaphore_signal(
            barrier, inc=1, device_id=(z, y, c, lax.rem(t + n, 4)), device_id_type=MESH
        )
    for n in range(1, 8):
        pl.semaphore_signal(barrier, inc=1, device_id=row_peer(n)[1], device_id_type=MESH)
    for n in range(1, 8):
        pl.semaphore_signal(barrier, inc=1, device_id=col_peer(n)[1], device_id_type=MESH)
    pl.semaphore_wait(barrier, 17)

    xr = Ring(x_buf, "tp", 0, 128, coords, (x_send, x_recv))
    kr = Ring(k_buf, "kv_0", 0, 4, coords, (k_send, k_recv))
    vr = Ring(v_buf, "kv_1", 0, 4, coords, (v_send, v_recv))
    orr = Ring(wo_buf, "tp", c * 192, 96, coords, (o_send, o_recv))

    locals_[0].wait()
    xr.start_own(0)
    xr.start_own(1)

    chosen = chosen_ref[...]
    lane = lax.broadcasted_iota(jnp.int32, (16, 512), 1)
    hit_all = jnp.zeros((16, 512), jnp.bool_)
    hit_own = jnp.zeros((16, 512), jnp.bool_)
    own_id = me * 16 + lane // 32
    for e in range(SEL):
        col = chosen[:, e : e + 1]
        hit_all = hit_all | (col == lane)
        hit_own = hit_own | (col == own_id)
    lane8 = lax.broadcasted_iota(jnp.int32, (8, 512), 1)
    wanted = jnp.max(jnp.where(hit_all & (lane // 16 != me), 1, 0), axis=0, keepdims=True)
    wanted = jnp.broadcast_to(wanted, (8, 512))
    place = lane8 % 16

    def scan(value):
        for step in (1, 2, 4, 8):
            value = value + jnp.where(place >= step, pltpu.roll(value, step, 1), 0)
        return value

    count = scan(wanted)
    first = scan(jnp.where((wanted == 1) & (count == 1), place + 1, 0))
    second = scan(jnp.where((wanted == 1) & (count == 2), place + 1, 0))
    asked = jnp.where(place == 15, first, jnp.where(place == 14, pltpu.roll(second, 511, 1), 0))
    row = jnp.maximum(asked - 1, 0)
    req_row[pl.ds(yc, 1)] = row.reshape(1, 8, 512)
    req_col[pl.ds(zc, 1)] = row.reshape(1, 8, 512)
    ti = lax.broadcasted_iota(jnp.int32, (512, 512), 0)
    tj = lax.broadcasted_iota(jnp.int32, (512, 512), 1)
    asked_f = asked.astype(F32).astype(BF16)
    source = (tj // 64) * 16 + 15 - (tj // 32) % 2
    for g in range(4):
        spread = jnp.where(ti == g * 128 + source, 1.0, 0.0).astype(BF16)
        value = dot(asked_f, spread).astype(jnp.int32)
        ids = jnp.where(value > 0, (g * 8 + lane8 // 64) * 16 + value - 1, -1)[0:1]
        hit = jnp.zeros((16, 512), jnp.bool_)
        for e in range(SEL):
            hit = hit | (chosen[:, e : e + 1] == ids)
        bias_far[g] = jnp.where(hit, 0.0, NEG)
    own_row = jnp.where(hit_own, 0.0, NEG)
    seen = jnp.broadcast_to(own_row[:, None, :], (16, 32, 512)).reshape(512, 512)
    bias_own[...] = jnp.where(tj <= ti, seen, NEG)

    req_sent = []
    for n in range(1, 8):
        for which, buf, mine, peer in ((0, req_row, yc, row_peer), (1, req_col, zc, col_peer)):
            copy = pltpu.make_async_remote_copy(
                src_ref=buf.at[mine],
                dst_ref=buf.at[mine],
                send_sem=req_send.at[which, n],
                recv_sem=req_recv.at[which, n],
                device_id=peer(n)[1],
                device_id_type=MESH,
            )
            copy.start()
            req_sent.append(copy)

    for copy in locals_[1:4]:
        copy.wait()

    for i in range(CHUNKS):
        rows = slice(i * 128, (i + 1) * 128)
        xr.wait_sides(i)
        xr.forward(i)
        if i + 2 < CHUNKS:
            xr.start_own(i + 2)
        if i >= 1:
            for ring in (kr, vr):
                ring.start_own(i - 1)
        acc = dot(x_buf[t, rows, :], w_buf[t])
        acc = acc + dot(x_buf[xr.left, rows, :], w_buf[xr.left])
        acc = acc + dot(x_buf[xr.right, rows, :], w_buf[xr.right])
        if i >= 2:
            for ring in (kr, vr):
                ring.wait_sides(i - 2)
                ring.forward(i - 2)
        xr.wait_opp(i)
        acc = acc + dot(x_buf[xr.opp, rows, :], w_buf[xr.opp])
        q_buf[rows, :] = (acc[:, 0:384] * (HD**-0.5 * LOG2E)).astype(BF16)
        blocks = slice(i * 4, (i + 1) * 4)
        k_buf[pl.ds(z, 1), blocks] = acc[:, 384:768].astype(BF16).reshape(1, 4, 32, 384)
        v_buf[pl.ds(y, 1), blocks] = acc[:, 768:1152].astype(BF16).reshape(1, 4, 32, 384)

    for n in range(1, 8):
        for which, buf, peer in ((0, req_row, row_peer), (1, req_col, col_peer)):
            j = peer(8 - n)[0]
            pltpu.make_async_remote_copy(
                src_ref=buf.at[j],
                dst_ref=buf.at[j],
                send_sem=req_send.at[which, n],
                recv_sem=req_recv.at[which, n],
                device_id=peer(n)[1],
                device_id_type=MESH,
            ).wait_recv()
    to_smem = [
        pltpu.make_async_copy(req_row.at[:, 0], smem_row, local_sem.at[5]),
        pltpu.make_async_copy(req_col.at[:, 0], smem_col, local_sem.at[6]),
    ]
    for copy in to_smem:
        copy.start()
    for ring in (kr, vr):
        ring.start_own(CHUNKS - 1)
    locals_[4].wait()
    orr.start_own(0)
    orr.start_own(1)
    for copy in to_smem:
        copy.wait()

    m_buf[...] = jnp.full(m_buf.shape, NEG, F32)
    l_buf[...] = jnp.zeros(l_buf.shape, F32)
    acc_buf[...] = jnp.zeros(acc_buf.shape, F32)

    def attend(k_all, v_all, bias):
        for h in range(3):
            cols = slice(h * HD, (h + 1) * HD)
            s = bias(dot_t(q_buf[:, cols], k_all[:, cols]))
            m_old = m_buf[h]
            m_new = jnp.maximum(m_old, jnp.max(s, axis=-1, keepdims=True))
            p = jnp.exp2(s - m_new)
            scale = jnp.exp2(m_old - m_new)
            m_buf[h] = m_new
            l_buf[h] = l_buf[h] * scale + jnp.sum(p, axis=-1, keepdims=True)
            acc_buf[h] = acc_buf[h] * scale + dot(p.astype(BF16), v_all[:, cols])

    for i in (CHUNKS - 2, CHUNKS - 1):
        for ring in (kr, vr):
            ring.wait_sides(i)
            ring.forward(i)
    attend(k_buf[z].reshape(512, 384), v_buf[y].reshape(512, 384), lambda s: s + bias_own[...])
    for i in range(CHUNKS):
        for ring in (kr, vr):
            ring.wait_opp(i)

    slot_sent = []

    def slot_k(n, g):
        j, device = row_peer(n)
        return pltpu.make_async_remote_copy(
            src_ref=stk.at[g, j],
            dst_ref=fark.at[g, yc],
            send_sem=ks_send.at[g, n],
            recv_sem=ks_recv.at[g, n],
            device_id=device,
            device_id_type=MESH,
        )

    def slot_v(n):
        j, device = col_peer(n)
        return pltpu.make_async_remote_copy(
            src_ref=stv.at[j],
            dst_ref=farv.at[z, :, c],
            send_sem=vs_send.at[n],
            recv_sem=vs_recv.at[n],
            device_id=device,
            device_id_type=MESH,
        )

    def wait_k(n, g):
        j = row_peer(8 - n)[0]
        pltpu.make_async_remote_copy(
            src_ref=stk.at[g, j],
            dst_ref=fark.at[g, j],
            send_sem=ks_send.at[g, n],
            recv_sem=ks_recv.at[g, n],
            device_id=row_peer(n)[1],
            device_id_type=MESH,
        ).wait_recv()

    def wait_v(n):
        j = col_peer(8 - n)[0]
        pltpu.make_async_remote_copy(
            src_ref=stv.at[j],
            dst_ref=farv.at[j // 2, :, lax.rem(j, 2)],
            send_sem=vs_send.at[n],
            recv_sem=vs_recv.at[n],
            device_id=col_peer(n)[1],
            device_id_type=MESH,
        ).wait_recv()

    def stage_v(j, carry):
        for s in range(4):
            for k in range(2):
                b = smem_col[j, (z * 8 + s * 2 + c) * 16 + 15 - k]
                stv[j, s, pl.ds(k * BLK, BLK), :] = v_buf[s, b]
        return carry

    lax.fori_loop(0, 8, stage_v, 0)

    def stage_k(j, carry):
        for g in range(4):
            for k in range(2):
                b = smem_row[j, (g * 8 + yc) * 16 + 15 - k]
                stk[g, j, pl.ds(k * BLK, BLK), :] = k_buf[g, b]
        return carry

    lax.fori_loop(0, 8, stage_k, 0)
    order = (4, 5, 3, 2, 6, 7, 1)
    for g in range(4):
        for n in order:
            copy = slot_k(n, g)
            copy.start()
            slot_sent.append(copy)
        if g == 0:
            for n in order:
                copy = slot_v(n)
                copy.start()
                slot_sent.append(copy)
    for g in range(4):
        fark[g, pl.ds(yc, 1)] = stk[g, pl.ds(yc, 1)]
    for s in range(4):
        farv[pl.ds(z, 1), s, pl.ds(c, 1)] = stv[pl.ds(zc, 1), s].reshape(1, 1, 64, 384)

    for i in range(2):
        orr.wait_sides(i)
        orr.forward(i)

    for n in range(1, 8):
        wait_v(n)
    for g in range(4):
        for n in range(1, 8):
            wait_k(n, g)

    def far(g, carry):
        bias = bias_far[g]
        attend(
            fark[g].reshape(512, 384),
            farv[g].reshape(512, 384),
            lambda s: (s.reshape(16, 32, 512) + bias[:, None, :]).reshape(512, 512),
        )
        return carry

    lax.fori_loop(0, z + 1, far, 0)

    for i in range(2):
        orr.wait_opp(i)
    partner = (z, y, 1 - c, t)
    d2d = []
    for n in range(1, 4):
        s = lax.rem(t + n, 4)
        copy = pltpu.make_async_remote_copy(
            src_ref=wo_buf.at[s, pl.ds(c * 192, 192), :],
            dst_ref=wo_buf.at[s, pl.ds(c * 192, 192), :],
            send_sem=d_send.at[n],
            recv_sem=d_recv.at[n],
            device_id=partner,
            device_id_type=MESH,
        )
        copy.start()
        d2d.append(copy)

    for h in range(3):
        cols = slice(h * HD, (h + 1) * HD)
        att_buf[:, cols] = (acc_buf[h] / l_buf[h]).astype(BF16)

    a_sent = []
    for n in (2, 1, 3):
        s = lax.rem(t + n, 4)
        copy = pltpu.make_async_remote_copy(
            src_ref=att_buf.at[pl.ds(s * 128, 128), :],
            dst_ref=attx.at[t],
            send_sem=a_send.at[n],
            recv_sem=a_recv.at[n],
            device_id=(z, y, c, s),
            device_id_type=MESH,
        )
        copy.start()
        a_sent.append(copy)

    total = dot(att_buf[pl.ds(pl.multiple_of(t * 128, 128), 128), :], wo_buf[t])
    for n in (1, 3, 2):
        s = lax.rem(t + n, 4)
        pltpu.make_async_remote_copy(
            src_ref=wo_buf.at[s, pl.ds((1 - c) * 192, 192), :],
            dst_ref=wo_buf.at[s, pl.ds((1 - c) * 192, 192), :],
            send_sem=d_send.at[n],
            recv_sem=d_recv.at[n],
            device_id=partner,
            device_id_type=MESH,
        ).wait_recv()
        pltpu.make_async_remote_copy(
            src_ref=attx.at[s],
            dst_ref=attx.at[s],
            send_sem=a_send.at[4 - n],
            recv_sem=a_recv.at[4 - n],
            device_id=(z, y, c, s),
            device_id_type=MESH,
        ).wait_recv()
        total = total + dot(attx[s], wo_buf[s])
    out_ref[...] = total.astype(BF16)

    for ring in (xr, kr, vr, orr):
        ring.drain()
    for copy in req_sent + slot_sent + d2d + a_sent:
        copy.wait_send()


def local(tokens, w_query, w_key, w_value, w_out, chosen):
    any_ = pl.BlockSpec(memory_space=pl.ANY)
    vmem = pl.BlockSpec(memory_space=pltpu.VMEM)
    dma = pltpu.SemaphoreType.DMA
    return pl.pallas_call(
        body,
        out_shape=jax.ShapeDtypeStruct((128, 2048), BF16),
        in_specs=[any_] * 5 + [vmem],
        out_specs=vmem,
        scratch_shapes=[
            pltpu.VMEM((4, 512, 512), BF16),
            pltpu.VMEM((4, 512, 1152), BF16),
            pltpu.VMEM((512, 384), BF16),
            pltpu.VMEM((4, 16, 32, 384), BF16),
            pltpu.VMEM((4, 16, 32, 384), BF16),
            pltpu.VMEM((4, 384, 2048), BF16),
            pltpu.VMEM((4, 8, 64, 384), BF16),
            pltpu.VMEM((8, 4, 64, 384), BF16),
            pltpu.VMEM((4, 8, 64, 384), BF16),
            pltpu.VMEM((4, 4, 2, 64, 384), BF16),
            pltpu.VMEM((512, 384), BF16),
            pltpu.VMEM((4, 128, 384), BF16),
            pltpu.VMEM((512, 512), F32),
            pltpu.VMEM((4, 16, 512), F32),
            pltpu.VMEM((3, 512, 1), F32),
            pltpu.VMEM((3, 512, 1), F32),
            pltpu.VMEM((3, 512, 128), F32),
            pltpu.VMEM((8, 8, 512), jnp.int32),
            pltpu.VMEM((8, 8, 512), jnp.int32),
            pltpu.SMEM((8, 512), jnp.int32),
            pltpu.SMEM((8, 512), jnp.int32),
            dma((7,)),
            dma((2, 8)),
            dma((2, 8)),
            dma((4, 4)), dma((4, 4)), dma((4, 4)), dma((4, 4)),
            dma((4, 4)), dma((4, 4)), dma((4, 2)), dma((4, 2)),
            dma((4, 8)), dma((4, 8)), dma((8,)), dma((8,)),
            dma((4,)), dma((4,)), dma((4,)), dma((4,)),
        ],
        compiler_params=pltpu.CompilerParams(
            collective_id=0, has_side_effects=True, vmem_limit_bytes=60 * 1024 * 1024
        ),
        name="layer",
    )(
        tokens,
        w_query.reshape(4, 512, 384),
        w_key.reshape(4, 512, 384),
        w_value.reshape(4, 512, 384),
        w_out,
        chosen,
    )


def solution(mesh):
    finer = Mesh(mesh.devices.reshape(4, 4, 2, mesh.shape["tp"]), KV_TP)
    placed = (P(KV, "tp"), P(None, "tp"), P(None, "tp"), P(None, "tp"), P("tp", None), P(KV, None))
    return jax.shard_map(
        local, mesh=finer, in_specs=placed, out_specs=P(KV_TP, None), check_vma=False
    )
```

```python
import functools
import math

import jax
import jax.numpy as jnp
from jax import lax
from jax.experimental import pallas as pl
from jax.experimental.pallas import tpu as pltpu
from jax.sharding import Mesh
from jax.sharding import PartitionSpec as P

HD = 128
BLK = 32
SEL = 24
KV = ("kv_0", "kv_1", "kv_2")
KV_TP = ("kv_0", "kv_1", "kv_2", "tp")
NEG = -1e30
MESH = pl.DeviceIdType.MESH
F32 = jnp.float32
BF16 = jnp.bfloat16
SIZES = (4, 4, 4, 3, 1)
STARTS = (0, 4, 8, 12, 15)
CHUNKS = len(SIZES)
LOG2E = 1.4426950408889634


def dot(a, b):
    return jnp.dot(a, b, preferred_element_type=F32)


def dot_t(a, b):
    return lax.dot_general(a, b, (((1,), (1,)), ((), ())), preferred_element_type=F32)


def dot_0(a, b):
    return lax.dot_general(a, b, (((0,), (0,)), ((), ())), preferred_element_type=F32)


def sent_bytes(view, sem):
    pltpu.make_async_copy(view, view, sem).wait()


class Ring:
    def __init__(self, buf, axis, chunks, coords, sems):
        self.buf, self.axis, self.chunks = buf, axis, chunks
        self.me = coords[axis]
        self.right = lax.rem(self.me + 1, 4)
        self.left = lax.rem(self.me + 3, 4)
        self.opp = lax.rem(self.me + 2, 4)
        self.coords = coords
        self.send, self.recv = sems

    def _copy(self, slot, start, size, target, kind, i):
        view = self.buf.at[slot, pl.ds(start, size)]
        return pltpu.make_async_remote_copy(
            src_ref=view,
            dst_ref=view,
            send_sem=self.send,
            recv_sem=self.recv.at[kind, i],
            device_id=tuple(target if a == self.axis else self.coords[a] for a in KV_TP),
            device_id_type=MESH,
        )

    def _start(self, *args):
        self._copy(*args).start()

    def start_own(self, i):
        start, size = self.chunks[i]
        self._start(self.me, start, size, self.right, 0, i)
        self._start(self.me, start, size, self.left, 1, i)

    def wait_sides(self, i):
        start, size = self.chunks[i]
        self._copy(self.left, start, size, self.right, 0, i).wait_recv()
        self._copy(self.right, start, size, self.left, 1, i).wait_recv()

    def forward(self, i):
        start, size = self.chunks[i]
        half = size // 2
        self._start(self.left, start, half, self.right, 2, i)
        self._start(self.right, start + half, half, self.left, 3, i)

    def start_all(self, i):
        self.start_own(i)
        self._start(self.me, *self.chunks[i], self.opp, 2, i)

    def wait_all(self, i):
        self.wait_sides(i)
        self._copy(self.opp, *self.chunks[i], self.opp, 2, i).wait_recv()

    def wait_opp(self, i):
        start, size = self.chunks[i]
        half = size // 2
        self._copy(self.opp, start, half, self.right, 2, i).wait_recv()
        self._copy(self.opp, start + half, half, self.left, 3, i).wait_recv()

    def drain(self):
        start = self.chunks[0][0]
        size = sum(n for _, n in self.chunks)
        sent_bytes(self.buf.at[pl.ds(0, 3), pl.ds(start, size)], self.send)


def body(
    tok_hbm, wq_hbm, wk_hbm, wv_hbm, wo_hbm, chosen_ref,
    out_ref,
    x_buf, w_buf, q_buf, k_buf, v_buf, wo_buf,
    stk, stv, fark, farv, att_buf, attx,
    bias_own, bias_far, m_buf, l_buf, acc_buf,
    req_row, req_col, smem_row, smem_col,
    local_sem, req_send, req_recv,
    x_send, x_recv, k_send, k_recv, v_send, v_recv, o_send, o_recv,
    ks_send, ks_recv, vs_send, vs_recv, d_send, d_recv, a_send, a_recv,
):
    z, y, c, t = (lax.axis_index(a) for a in KV_TP)
    coords = dict(zip(KV_TP, (z, y, c, t)))
    me = z * 8 + y * 2 + c
    yc = y * 2 + c
    zc = z * 2 + c

    locals_ = [pltpu.make_async_copy(tok_hbm, x_buf.at[t], local_sem.at[0])]
    for n, w in enumerate((wq_hbm, wk_hbm, wv_hbm)):
        locals_.append(
            pltpu.make_async_copy(w, w_buf.at[:, :, pl.ds(n * 384, 384)], local_sem.at[1 + n])
        )
    locals_.append(pltpu.make_async_copy(wo_hbm, wo_buf.at[t], local_sem.at[4]))
    for copy in locals_:
        copy.start()

    def row_peer(n):
        j = lax.rem(yc + n, 8)
        return j, (z, j // 2, lax.rem(j, 2), t)

    def col_peer(n):
        j = lax.rem(zc + n, 8)
        return j, (j // 2, y, lax.rem(j, 2), t)

    barrier = pltpu.get_barrier_semaphore()
    for n in range(1, 4):
        pl.semaphore_signal(
            barrier, inc=1, device_id=(z, y, c, lax.rem(t + n, 4)), device_id_type=MESH
        )
    for n in range(1, 8):
        pl.semaphore_signal(barrier, inc=1, device_id=row_peer(n)[1], device_id_type=MESH)
    for n in range(1, 8):
        pl.semaphore_signal(barrier, inc=1, device_id=col_peer(n)[1], device_id_type=MESH)
    with jax.named_scope("barrier"):
        pl.semaphore_wait(barrier, 17)

    blocks = tuple(zip(STARTS, SIZES))
    xr = Ring(
        x_buf, "tp", tuple((p * BLK, n * BLK) for p, n in blocks), coords, (x_send, x_recv)
    )
    kr = Ring(k_buf, "kv_0", blocks, coords, (k_send, k_recv))
    vr = Ring(v_buf, "kv_1", blocks, coords, (v_send, v_recv))
    orr = Ring(wo_buf, "tp", ((c * 192, 96), (c * 192 + 96, 96)), coords, (o_send, o_recv))

    locals_[0].wait()
    xr.start_own(0)
    xr.start_own(1)

    with jax.named_scope("plan"):
        chosen = chosen_ref[...]
        lane = lax.broadcasted_iota(jnp.int32, (16, 512), 1)
        sub = lax.broadcasted_iota(jnp.int32, (16, 512), 0)
        hit_all = jnp.zeros((16, 512), jnp.bool_)
        for e in range(SEL):
            hit_all = hit_all | (chosen[:, e : e + 1] == lane)
        lane8 = lax.broadcasted_iota(jnp.int32, (8, 512), 1)
        wanted = jnp.max(jnp.where(hit_all & (lane // 16 != me), 1, 0), axis=0, keepdims=True)
        wanted = jnp.broadcast_to(wanted, (8, 512))
        place = lane8 % 16

        def scan(value):
            for step in (1, 2, 4, 8):
                value = value + jnp.where(place >= step, pltpu.roll(value, step, 1), 0)
            return value

        count = scan(wanted)
        first = scan(jnp.where((wanted == 1) & (count == 1), place + 1, 0))
        second = scan(jnp.where((wanted == 1) & (count == 2), place + 1, 0))
        asked = jnp.where(
            place == 15, first, jnp.where(place == 14, pltpu.roll(second, 511, 1), 0)
        )
        row = jnp.maximum(asked - 1, 0)
        req_row[pl.ds(yc, 1)] = row.reshape(1, 8, 512)
        req_col[pl.ds(zc, 1)] = row.reshape(1, 8, 512)

    for n in range(1, 8):
        for which, buf, mine, peer in ((0, req_row, yc, row_peer), (1, req_col, zc, col_peer)):
            copy = pltpu.make_async_remote_copy(
                src_ref=buf.at[mine],
                dst_ref=buf.at[mine],
                send_sem=req_send,
                recv_sem=req_recv.at[which],
                device_id=peer(n)[1],
                device_id_type=MESH,
            )
            copy.start()

    with jax.named_scope("masks"):
        widen = jnp.where(sub == lane // 32, 1.0, 0.0).astype(BF16)
        high = dot_0((chosen // 16).astype(F32).astype(BF16), widen)
        low = dot_0((chosen % 16).astype(F32).astype(BF16), widen)
        chosen_t = high.astype(jnp.int32) * 16 + low.astype(jnp.int32)
        asked_f = asked.astype(F32).astype(BF16)
        for g in range(5):
            if g < 4:
                spread = jnp.where(lane == (g * 8 + sub // 2) * 16 + 15 - sub % 2, 1.0, 0.0)
                value = dot_t(spread.astype(BF16), asked_f).astype(jnp.int32)[:, 0:1]
                sub1 = sub[:, 0:1]
                ids = jnp.where(value > 0, (g * 8 + sub1 // 2) * 16 + value - 1, -1)
                ids = jnp.broadcast_to(ids, (16, 512))
            else:
                ids = me * 16 + sub
            hit = jnp.zeros((16, 512), jnp.bool_)
            for e in range(SEL):
                hit = hit | (chosen_t[e : e + 1, :] == ids)
            bias_far[g] = jnp.where(hit, 0.0, NEG)
        ti = lax.broadcasted_iota(jnp.int32, (512, 512), 0)
        tj = lax.broadcasted_iota(jnp.int32, (512, 512), 1)
        seen = jnp.broadcast_to(bias_far[4][:, None, :], (16, 32, 512)).reshape(512, 512)
        bias_own[...] = jnp.where(ti <= tj, seen, NEG)
        m_buf[...] = jnp.full(m_buf.shape, NEG, F32)
        l_buf[...] = jnp.zeros(l_buf.shape, F32)
        acc_buf[...] = jnp.zeros(acc_buf.shape, F32)

    for copy in locals_[1:4]:
        copy.wait()

    def next_sides(i):
        with jax.named_scope("xsides"):
            xr.wait_sides(i)
        xr.forward(i)
        if i + 2 < CHUNKS:
            xr.start_own(i + 2)

    next_sides(0)
    for i in range(CHUNKS):
        first, size = blocks[i]
        rows = slice(first * BLK, (first + size) * BLK)
        if i >= 1:
            for ring in (kr, vr):
                ring.start_all(i - 1)
        acc = dot(x_buf[t, rows, :], w_buf[t])
        acc = acc + dot(x_buf[xr.left, rows, :], w_buf[xr.left])
        acc = acc + dot(x_buf[xr.right, rows, :], w_buf[xr.right])
        if i + 1 < CHUNKS:
            next_sides(i + 1)
        if i == 0:
            sent_bytes(req_row.at[pl.ds(0, 7)], req_recv.at[0])
            sent_bytes(req_col.at[pl.ds(0, 7)], req_recv.at[1])
            to_smem = [
                pltpu.make_async_copy(req_row.at[:, 0], smem_row, local_sem.at[5]),
                pltpu.make_async_copy(req_col.at[:, 0], smem_col, local_sem.at[6]),
            ]
            for copy in to_smem:
                copy.start()
        if i == 1:
            for copy in to_smem:
                copy.wait()
        with jax.named_scope("xopp"):
            xr.wait_opp(i)
        acc = acc + dot(x_buf[xr.opp, rows, :], w_buf[xr.opp])
        q_buf[rows, :] = (acc[:, 0:384] * (HD**-0.5 * LOG2E)).astype(BF16)
        k_buf[pl.ds(z, 1), first : first + size] = (
            acc[:, 384:768].astype(BF16).reshape(1, size, BLK, 384)
        )
        v_buf[pl.ds(y, 1), first : first + size] = (
            acc[:, 768:1152].astype(BF16).reshape(1, size, BLK, 384)
        )
    for ring in (kr, vr):
        ring.start_all(CHUNKS - 1)
    locals_[4].wait()
    orr.start_own(0)
    orr.start_own(1)
    with jax.named_scope("kvopp"):
        for i in range(CHUNKS):
            for ring in (kr, vr):
                ring.wait_all(i)

    def score(k_all, h):
        cols = slice(h * HD, (h + 1) * HD)
        return dot_t(k_all[:, cols], q_buf[:, cols])

    def attend(k_all, v_all, bias, done=None):
        later = score(k_all, 0)
        for h in range(3):
            s = later
            if h < 2:
                later = score(k_all, h + 1)
            s = bias(s)
            m_old = m_buf[h]
            m_new = jnp.maximum(m_old, jnp.max(s, axis=0, keepdims=True))
            p = jnp.exp2(s - m_new)
            scale = jnp.exp2(m_old - m_new)
            m_buf[h] = m_new
            total = l_buf[h] * scale + jnp.sum(p, axis=0, keepdims=True)
            l_buf[h] = total
            v = v_all[:, h * HD : (h + 1) * HD]
            mixed = acc_buf[h] * scale + dot_0(v, p.astype(BF16))
            acc_buf[h] = mixed
            if done is not None:
                done(h, mixed / total)

    def slot_k(n, step):
        j, device = row_peer(n)
        return pltpu.make_async_remote_copy(
            src_ref=stk.at[z - step, j],
            dst_ref=fark.at[z - step, yc],
            send_sem=ks_send.at[step],
            recv_sem=ks_recv.at[z - step],
            device_id=device,
            device_id_type=MESH,
        )

    def slot_v(n):
        j, device = col_peer(n)
        return pltpu.make_async_remote_copy(
            src_ref=stv.at[j],
            dst_ref=farv.at[z, :, c],
            send_sem=vs_send.at[n],
            recv_sem=vs_recv.at[n],
            device_id=device,
            device_id_type=MESH,
        )

    def wait_k(g):
        sent_bytes(fark.at[g, pl.ds(0, 7)], ks_recv.at[g])

    def wait_sent_k(step):
        sent_bytes(stk.at[0, pl.ds(0, 7)], ks_send.at[step])

    def wait_v(j):
        n = lax.rem(zc - j + 8, 8)
        pltpu.make_async_remote_copy(
            src_ref=stv.at[j],
            dst_ref=farv.at[j // 2, :, lax.rem(j, 2)],
            send_sem=vs_send.at[n],
            recv_sem=vs_recv.at[n],
            device_id=(j // 2, y, lax.rem(j, 2), t),
            device_id_type=MESH,
        ).wait_recv()

    def stage_v(j, carry):
        for s in range(4):
            for k in range(2):
                b = smem_col[j, (z * 8 + s * 2 + c) * 16 + 15 - k]
                stv[j, s, pl.ds(k * BLK, BLK), :] = v_buf[s, b]
        return carry

    with jax.named_scope("stagev"):
        lax.fori_loop(0, 8, stage_v, 0)

    def stage_k(j, carry):
        for g in range(4):
            for k in range(2):
                b = smem_row[j, (g * 8 + yc) * 16 + 15 - k]
                stk[g, j, pl.ds(k * BLK, BLK), :] = k_buf[g, b]
        return carry

    with jax.named_scope("stagek"):
        lax.fori_loop(0, 8, stage_k, 0)
    order = (4, 5, 3, 2, 6, 7, 1)

    def send_v(n):
        @pl.when(col_peer(n)[0] // 2 >= z)
        def _():
            slot_v(n).start()

    def send_k(step):
        @pl.when(step <= z)
        def _():
            for n in order:
                slot_k(n, step).start()

    with jax.named_scope("sends"):
        send_k(0)
        for n in (1, 2, 3, 6, 7, 4, 5):
            send_v(n)
        send_k(1)
    for g in range(4):
        fark[g, pl.ds(yc, 1)] = stk[g, pl.ds(yc, 1)]
    for s in range(4):
        farv[pl.ds(z, 1), s, pl.ds(c, 1)] = stv[pl.ds(zc, 1), s].reshape(1, 1, 64, 384)

    with jax.named_scope("own"):
        attend(
            k_buf[z].reshape(512, 384), v_buf[y].reshape(512, 384), lambda s: s + bias_own[...]
        )
    with jax.named_scope("drain1"):
        for ring in (xr, kr, vr):
            ring.drain()
        sent_bytes(req_row.at[pl.ds(0, 7)], req_send)
        sent_bytes(req_row.at[pl.ds(0, 7)], req_send)

    def hand(slot, start, size):
        view = wo_buf.at[slot, pl.ds(c * 192 + start, size)]
        pltpu.make_async_remote_copy(
            src_ref=view,
            dst_ref=view,
            send_sem=d_send,
            recv_sem=d_recv,
            device_id=(z, y, 1 - c, t),
            device_id_type=MESH,
        ).start()

    def out_sides(i):
        with jax.named_scope("osides"):
            orr.wait_sides(i)
        orr.forward(i)
        for slot in (orr.left, orr.right):
            hand(slot, i * 96, 96)

    out_sides(0)

    def far_parts(g):
        bias = bias_far[g]
        return (
            fark[g].reshape(512, 384),
            farv[g].reshape(512, 384),
            lambda s: (s.reshape(16, 32, 512) + bias[:, None, :]).reshape(512, 512),
        )

    def wait_group(g):
        with jax.named_scope("wk"):
            wait_k(g)
        with jax.named_scope("wv"):
            for core in range(2):

                @pl.when(g * 2 + core != zc)
                def _():
                    wait_v(g * 2 + core)

    def group(step):
        @pl.when(step < z)
        def _():
            with jax.named_scope("ksent"):
                wait_sent_k(step)
            if step + 2 < 4:
                send_k(step + 2)
            wait_group(z - step)
            with jax.named_scope("far"):
                attend(*far_parts(z - step))

    group(0)
    group(1)
    out_sides(1)
    group(2)
    with jax.named_scope("oopp"):
        for i in range(2):
            orr.wait_opp(i)
            hand(orr.opp, i * 96, 96)

    def share(h, n):
        s = lax.rem(t + n, 4)
        cols = pl.ds(h * HD, HD)
        return pltpu.make_async_remote_copy(
            src_ref=att_buf.at[pl.ds(s * 128, 128), cols],
            dst_ref=attx.at[t, :, cols],
            send_sem=a_send,
            recv_sem=a_recv.at[n],
            device_id=(z, y, c, s),
            device_id_type=MESH,
        )

    def finish(h, attended):
        att_buf[:, h * HD : (h + 1) * HD] = attended.T.astype(BF16)
        for n in (2, 1, 3):
            share(h, n).start()

    wait_group(0)
    with jax.named_scope("lastfar"):
        attend(*far_parts(lax.div(me, 32)), done=finish)

    total = dot(att_buf[pl.ds(pl.multiple_of(t * 128, 128), 128), :], wo_buf[t])
    with jax.named_scope("handed"):
        sent_bytes(wo_buf.at[pl.ds(0, 3), pl.ds((1 - c) * 192, 192)], d_recv)
    for n in (1, 3, 2):
        s = lax.rem(t + n, 4)
        with jax.named_scope("awaited"):
            sent_bytes(attx.at[s], a_recv.at[4 - n])
        with jax.named_scope("outn"):
            total = total + dot(attx[s], wo_buf[s])
    out_ref[...] = total.astype(BF16)

    with jax.named_scope("drain2"):
        orr.drain()
        sent_bytes(wo_buf.at[pl.ds(0, 3), pl.ds(c * 192, 192)], d_send)
        sent_bytes(attx.at[pl.ds(0, 3)], a_send)
        wait_sent_k(z)
        for n in order:

            @pl.when(col_peer(n)[0] // 2 >= z)
            def _():
                slot_v(n).wait_send()


def local(tokens, w_query, w_key, w_value, w_out, chosen):
    any_ = pl.BlockSpec(memory_space=pltpu.HBM)
    vmem = pl.BlockSpec(memory_space=pltpu.VMEM)
    dma = pltpu.SemaphoreType.DMA
    return pl.pallas_call(
        body,
        out_shape=jax.ShapeDtypeStruct((128, 2048), BF16),
        in_specs=[any_] * 5 + [vmem],
        out_specs=vmem,
        scratch_shapes=[
            pltpu.VMEM((4, 512, 512), BF16),
            pltpu.VMEM((4, 512, 1152), BF16),
            pltpu.VMEM((512, 384), BF16),
            pltpu.VMEM((4, 16, 32, 384), BF16),
            pltpu.VMEM((4, 16, 32, 384), BF16),
            pltpu.VMEM((4, 384, 2048), BF16),
            pltpu.VMEM((4, 8, 64, 384), BF16),
            pltpu.VMEM((8, 4, 64, 384), BF16),
            pltpu.VMEM((4, 8, 64, 384), BF16),
            pltpu.VMEM((4, 4, 2, 64, 384), BF16),
            pltpu.VMEM((512, 384), BF16),
            pltpu.VMEM((4, 128, 384), BF16),
            pltpu.VMEM((512, 512), F32),
            pltpu.VMEM((5, 16, 512), F32),
            pltpu.VMEM((3, 1, 512), F32),
            pltpu.VMEM((3, 1, 512), F32),
            pltpu.VMEM((3, 128, 512), F32),
            pltpu.VMEM((8, 8, 512), jnp.int32),
            pltpu.VMEM((8, 8, 512), jnp.int32),
            pltpu.SMEM((8, 512), jnp.int32),
            pltpu.SMEM((8, 512), jnp.int32),
            dma((7,)),
            dma,
            dma((2,)),
            dma, dma((4, CHUNKS)), dma, dma((4, CHUNKS)),
            dma, dma((4, CHUNKS)), dma, dma((4, 2)),
            dma((4,)), dma((4,)), dma((8,)), dma((8,)),
            dma, dma, dma, dma((4,)),
        ],
        compiler_params=pltpu.CompilerParams(
            collective_id=0, has_side_effects=True, vmem_limit_bytes=56_000_000
        ),
        name="layer",
    )(
        tokens,
        w_query.reshape(4, 512, 384),
        w_key.reshape(4, 512, 384),
        w_value.reshape(4, 512, 384),
        w_out,
        chosen,
    )


def solution(mesh):
    finer = Mesh(mesh.devices.reshape(4, 4, 2, mesh.shape["tp"]), KV_TP)
    placed = (P(KV, "tp"), P(None, "tp"), P(None, "tp"), P(None, "tp"), P("tp", None), P(KV, None))
    return jax.shard_map(
        local, mesh=finer, in_specs=placed, out_specs=P(KV_TP, None), check_vma=False
    )
```

```python
import functools
import math

import jax
import jax.numpy as jnp
from jax import lax
from jax.experimental import pallas as pl
from jax.experimental.pallas import tpu as pltpu
from jax.sharding import Mesh
from jax.sharding import PartitionSpec as P

HD = 128
BLK = 32
SEL = 24
KV = ("kv_0", "kv_1", "kv_2")
KV_TP = ("kv_0", "kv_1", "kv_2", "tp")
NEG = -1e30
MESH = pl.DeviceIdType.MESH
F32 = jnp.float32
BF16 = jnp.bfloat16
SIZES = (4, 4, 4, 3, 1)
STARTS = (0, 4, 8, 12, 15)
CHUNKS = len(SIZES)
PASSED = 2
AHEAD = 5
LOG2E = 1.4426950408889634


def dot(a, b):
    return jnp.dot(a, b, preferred_element_type=F32)


def dot_t(a, b):
    return lax.dot_general(a, b, (((1,), (1,)), ((), ())), preferred_element_type=F32)


def dot_0(a, b):
    return lax.dot_general(a, b, (((0,), (0,)), ((), ())), preferred_element_type=F32)


def sent_bytes(view, sem):
    pltpu.make_async_copy(view, view, sem).wait()


class Ring:
    def __init__(self, buf, axis, chunks, coords, sems, grain=1):
        self.buf, self.axis, self.chunks, self.grain = buf, axis, chunks, grain
        self.me = coords[axis]
        self.right = lax.rem(self.me + 1, 4)
        self.left = lax.rem(self.me + 3, 4)
        self.opp = lax.rem(self.me + 2, 4)
        self.coords = coords
        self.send, self.recv = sems

    def _copy(self, slot, start, size, target, kind, i):
        view = self.buf.at[slot, pl.ds(start, size)]
        return pltpu.make_async_remote_copy(
            src_ref=view,
            dst_ref=view,
            send_sem=self.send,
            recv_sem=self.recv.at[kind, i],
            device_id=tuple(target if a == self.axis else self.coords[a] for a in KV_TP),
            device_id_type=MESH,
        )

    def _start(self, *args):
        self._copy(*args).start()

    def start_own(self, i):
        start, size = self.chunks[i]
        self._start(self.me, start, size, self.right, 0, i)
        self._start(self.me, start, size, self.left, 1, i)

    def wait_sides(self, i):
        start, size = self.chunks[i]
        self._copy(self.left, start, size, self.right, 0, i).wait_recv()
        self._copy(self.right, start, size, self.left, 1, i).wait_recv()

    def half(self, size):
        return -(-size // (2 * self.grain)) * self.grain

    def forward(self, i):
        start, size = self.chunks[i]
        half = self.half(size)
        self._start(self.left, start, half, self.right, 2, i)
        self._start(self.right, start + half, size - half, self.left, 3, i)

    def start_all(self, i):
        self.start_own(i)
        self._start(self.me, *self.chunks[i], self.opp, 2, i)

    def wait_all(self, i):
        self.wait_sides(i)
        self._copy(self.opp, *self.chunks[i], self.opp, 2, i).wait_recv()

    def wait_opp(self, i):
        start, size = self.chunks[i]
        half = self.half(size)
        self._copy(self.opp, start, half, self.right, 2, i).wait_recv()
        self._copy(self.opp, start + half, size - half, self.left, 3, i).wait_recv()

    def drain(self):
        start = self.chunks[0][0]
        size = sum(n for _, n in self.chunks)
        sent_bytes(self.buf.at[pl.ds(0, 3), pl.ds(start, size)], self.send)


def body(
    tok_hbm, wq_hbm, wk_hbm, wv_hbm, wo_hbm, chosen_ref,
    out_ref,
    x_buf, w_buf, q_buf, k_buf, v_buf, wo_buf,
    stk, stv, fark, farv, att_buf, attx,
    bias_own, bias_far, m_buf, l_buf, acc_buf,
    req_row, req_col, smem_row, smem_col,
    local_sem, req_send, req_recv,
    x_send, x_recv, k_send, k_recv, v_send, v_recv, o_send, o_recv,
    ks_send, ks_recv, vs_send, vs_recv, d_send, d_recv, a_send, a_recv,
):
    z, y, c, t = (lax.axis_index(a) for a in KV_TP)
    coords = dict(zip(KV_TP, (z, y, c, t)))
    me = z * 8 + y * 2 + c
    yc = y * 2 + c
    zc = z * 2 + c

    locals_ = [pltpu.make_async_copy(tok_hbm, x_buf.at[t], local_sem.at[0])]
    for n, w in enumerate((wq_hbm, wk_hbm, wv_hbm)):
        locals_.append(
            pltpu.make_async_copy(w, w_buf.at[:, :, pl.ds(n * 384, 384)], local_sem.at[1 + n])
        )
    locals_.append(pltpu.make_async_copy(wo_hbm, wo_buf.at[t], local_sem.at[4]))
    for copy in locals_:
        copy.start()

    def row_peer(n):
        j = lax.rem(yc + n, 8)
        return j, (z, j // 2, lax.rem(j, 2), t)

    def col_peer(n):
        j = lax.rem(zc + n, 8)
        return j, (j // 2, y, lax.rem(j, 2), t)

    barrier = pltpu.get_barrier_semaphore()
    for n in range(1, 4):
        pl.semaphore_signal(
            barrier, inc=1, device_id=(z, y, c, lax.rem(t + n, 4)), device_id_type=MESH
        )
    for n in range(1, 8):
        pl.semaphore_signal(barrier, inc=1, device_id=row_peer(n)[1], device_id_type=MESH)
    for n in range(1, 8):
        pl.semaphore_signal(barrier, inc=1, device_id=col_peer(n)[1], device_id_type=MESH)
    with jax.named_scope("barrier"):
        pl.semaphore_wait(barrier, 17)

    blocks = tuple(zip(STARTS, SIZES))
    xr = Ring(
        x_buf, "tp", tuple((p * BLK, n * BLK) for p, n in blocks), coords, (x_send, x_recv)
    )
    kr = Ring(k_buf, "kv_0", blocks, coords, (k_send, k_recv))
    vr = Ring(v_buf, "kv_1", blocks, coords, (v_send, v_recv))
    base = c * 192
    outs = ((0, 96), (96, 96))
    orr = Ring(
        wo_buf, "tp", tuple((base + p, n) for p, n in outs), coords, (o_send, o_recv), grain=16
    )

    locals_[0].wait()
    xr.start_own(0)
    xr.start_own(1)

    with jax.named_scope("plan"):
        chosen = chosen_ref[...]
        lane = lax.broadcasted_iota(jnp.int32, (16, 512), 1)
        sub = lax.broadcasted_iota(jnp.int32, (16, 512), 0)
        hit_all = jnp.zeros((16, 512), jnp.bool_)
        for e in range(SEL):
            hit_all = hit_all | (chosen[:, e : e + 1] == lane)
        lane8 = lax.broadcasted_iota(jnp.int32, (8, 512), 1)
        wanted = jnp.max(jnp.where(hit_all & (lane // 16 != me), 1, 0), axis=0, keepdims=True)
        wanted = jnp.broadcast_to(wanted, (8, 512))
        place = lane8 % 16

        def scan(value):
            for step in (1, 2, 4, 8):
                value = value + jnp.where(place >= step, pltpu.roll(value, step, 1), 0)
            return value

        count = scan(wanted)
        first = scan(jnp.where((wanted == 1) & (count == 1), place + 1, 0))
        second = scan(jnp.where((wanted == 1) & (count == 2), place + 1, 0))
        asked = jnp.where(
            place == 15, first, jnp.where(place == 14, pltpu.roll(second, 511, 1), 0)
        )
        row = jnp.maximum(asked - 1, 0)
        req_row[pl.ds(yc, 1)] = row.reshape(1, 8, 512)
        req_col[pl.ds(zc, 1)] = row.reshape(1, 8, 512)

    for n in range(1, 8):
        for which, buf, mine, peer in ((0, req_row, yc, row_peer), (1, req_col, zc, col_peer)):
            copy = pltpu.make_async_remote_copy(
                src_ref=buf.at[mine],
                dst_ref=buf.at[mine],
                send_sem=req_send,
                recv_sem=req_recv.at[which],
                device_id=peer(n)[1],
                device_id_type=MESH,
            )
            copy.start()

    with jax.named_scope("masks"):
        widen = jnp.where(sub == lane // 32, 1.0, 0.0).astype(BF16)
        high = dot_0((chosen // 16).astype(F32).astype(BF16), widen)
        low = dot_0((chosen % 16).astype(F32).astype(BF16), widen)
        chosen_t = high.astype(jnp.int32) * 16 + low.astype(jnp.int32)
        asked_f = asked.astype(F32).astype(BF16)
        for g in range(5):
            if g < 4:
                spread = jnp.where(lane == (g * 8 + sub // 2) * 16 + 15 - sub % 2, 1.0, 0.0)
                value = dot_t(spread.astype(BF16), asked_f).astype(jnp.int32)[:, 0:1]
                sub1 = sub[:, 0:1]
                ids = jnp.where(value > 0, (g * 8 + sub1 // 2) * 16 + value - 1, -1)
                ids = jnp.broadcast_to(ids, (16, 512))
            else:
                ids = me * 16 + sub
            hit = jnp.zeros((16, 512), jnp.bool_)
            for e in range(SEL):
                hit = hit | (chosen_t[e : e + 1, :] == ids)
            bias_far[g] = jnp.where(hit, 0.0, NEG)
        ti = lax.broadcasted_iota(jnp.int32, (512, 512), 0)
        tj = lax.broadcasted_iota(jnp.int32, (512, 512), 1)
        seen = jnp.broadcast_to(bias_far[4][:, None, :], (16, 32, 512)).reshape(512, 512)
        bias_own[...] = jnp.where(ti <= tj, seen, NEG)
        m_buf[...] = jnp.full(m_buf.shape, NEG, F32)
        l_buf[...] = jnp.zeros(l_buf.shape, F32)
        acc_buf[...] = jnp.zeros(acc_buf.shape, F32)

    for copy in locals_[1:4]:
        copy.wait()

    def next_sides(i):
        with jax.named_scope("xsides"):
            xr.wait_sides(i)
        xr.forward(i)
        if i + 2 < CHUNKS:
            xr.start_own(i + 2)

    next_sides(0)
    for i in range(CHUNKS):
        first, size = blocks[i]
        rows = slice(first * BLK, (first + size) * BLK)
        if i >= 1:
            for ring in (kr, vr):
                (ring.start_own if i - 1 < PASSED else ring.start_all)(i - 1)
        acc = dot(x_buf[t, rows, :], w_buf[t])
        acc = acc + dot(x_buf[xr.left, rows, :], w_buf[xr.left])
        acc = acc + dot(x_buf[xr.right, rows, :], w_buf[xr.right])
        if i + 1 < CHUNKS:
            next_sides(i + 1)
        if i + 2 == CHUNKS:
            locals_[4].wait()
            orr.start_own(0)
        if i == 0:
            sent_bytes(req_row.at[pl.ds(0, 7)], req_recv.at[0])
            sent_bytes(req_col.at[pl.ds(0, 7)], req_recv.at[1])
            to_smem = [
                pltpu.make_async_copy(req_row.at[:, 0], smem_row, local_sem.at[5]),
                pltpu.make_async_copy(req_col.at[:, 0], smem_col, local_sem.at[6]),
            ]
            for copy in to_smem:
                copy.start()
        if i == 1:
            for copy in to_smem:
                copy.wait()
        if 0 <= i - 3 < PASSED:
            with jax.named_scope("kvsides"):
                for ring in (kr, vr):
                    ring.wait_sides(i - 3)
                    ring.forward(i - 3)
        with jax.named_scope("xopp"):
            xr.wait_opp(i)
        acc = acc + dot(x_buf[xr.opp, rows, :], w_buf[xr.opp])
        q_buf[rows, :] = (acc[:, 0:384] * (HD**-0.5 * LOG2E)).astype(BF16)
        k_buf[pl.ds(z, 1), first : first + size] = (
            acc[:, 384:768].astype(BF16).reshape(1, size, BLK, 384)
        )
        v_buf[pl.ds(y, 1), first : first + size] = (
            acc[:, 768:1152].astype(BF16).reshape(1, size, BLK, 384)
        )
    for ring in (kr, vr):
        ring.start_all(CHUNKS - 1)
    orr.start_own(1)
    with jax.named_scope("kvopp"):
        for i in range(CHUNKS):
            for ring in (kr, vr):
                (ring.wait_opp if i < PASSED else ring.wait_all)(i)

    def score(k, h):
        return dot_t(k, q_buf[:, h * HD : (h + 1) * HD])

    def absorb(h, s, v):
        m_old = m_buf[h]
        m_new = jnp.maximum(m_old, jnp.max(s, axis=0, keepdims=True))
        p = jnp.exp2(s - m_new)
        scale = jnp.exp2(m_old - m_new)
        m_buf[h] = m_new
        l_buf[h] = l_buf[h] * scale + jnp.sum(p, axis=0, keepdims=True)
        acc_buf[h] = acc_buf[h] * scale + dot_0(v, p.astype(BF16))

    def slot_k(n, unit):
        h, step = divmod(unit, 4)
        j, device = row_peer(n)
        return pltpu.make_async_remote_copy(
            src_ref=stk.at[z - step, h, j],
            dst_ref=fark.at[z - step, h, yc],
            send_sem=ks_send.at[unit],
            recv_sem=ks_recv.at[z - step, h],
            device_id=device,
            device_id_type=MESH,
        )

    def send_k(unit):
        @pl.when(unit % 4 <= z)
        def _():
            for n in order:
                slot_k(n, unit).start()

    def wait_sent_k(unit):
        @pl.when(unit % 4 <= z)
        def _():
            sent_bytes(stk.at[0, 0, pl.ds(0, 7)], ks_send.at[unit])

    def slot_v(n, h):
        j, device = col_peer(n)
        return pltpu.make_async_remote_copy(
            src_ref=stv.at[j, h],
            dst_ref=farv.at[z, h, :, c],
            send_sem=vs_send.at[h, n],
            recv_sem=vs_recv.at[h, n],
            device_id=device,
            device_id_type=MESH,
        )

    def each_v(action):
        for n in (1, 2, 3, 6, 7, 4, 5):

            @pl.when(col_peer(n)[0] // 2 >= z)
            def _():
                action(n)

    def wait_v(j, h):
        n = lax.rem(zc - j + 8, 8)
        pltpu.make_async_remote_copy(
            src_ref=stv.at[j, h],
            dst_ref=farv.at[j // 2, h, :, lax.rem(j, 2)],
            send_sem=vs_send.at[h, n],
            recv_sem=vs_recv.at[h, n],
            device_id=(j // 2, y, lax.rem(j, 2), t),
            device_id_type=MESH,
        ).wait_recv()

    def stage_v(j, carry):
        for s in range(4):
            for k in range(2):
                b = smem_col[j, (z * 8 + s * 2 + c) * 16 + 15 - k]
                block = v_buf[s, b]
                for h in range(3):
                    stv[j, h, s, pl.ds(k * BLK, BLK), :] = block[:, h * HD : (h + 1) * HD]
        return carry

    def stage_k(j, carry):
        for g in range(4):
            for k in range(2):
                b = smem_row[j, (g * 8 + yc) * 16 + 15 - k]
                block = k_buf[g, b]
                for h in range(3):
                    stk[g, h, j, pl.ds(k * BLK, BLK), :] = block[:, h * HD : (h + 1) * HD]
        return carry

    order = (4, 5, 3, 2, 6, 7, 1)
    with jax.named_scope("stage"):
        lax.fori_loop(0, 8, stage_k, 0)
        lax.fori_loop(0, 8, stage_v, 0)
    with jax.named_scope("sends"):
        send_k(0)
        each_v(lambda n: slot_v(n, 0).start())
        send_k(1)
        for unit in range(2, AHEAD):
            send_k(unit)
    for h in range(3):
        for g in range(4):
            fark[g, h, pl.ds(yc, 1)] = stk[g, h, pl.ds(yc, 1)]
        for s in range(4):
            farv[pl.ds(z, 1), h, s, pl.ds(c, 1)] = stv[pl.ds(zc, 1), h, s].reshape(1, 1, 64, HD)

    with jax.named_scope("own"):
        k_own = k_buf[z].reshape(512, 384)
        v_own = v_buf[y].reshape(512, 384)
        later = score(k_own[:, 0:HD], 0)
        for h in range(3):
            s = later + bias_own[...]
            if h < 2:
                later = score(k_own[:, (h + 1) * HD : (h + 2) * HD], h + 1)
            absorb(h, s, v_own[:, h * HD : (h + 1) * HD])
    with jax.named_scope("drain1"):
        for ring in (xr, kr, vr):
            ring.drain()
        sent_bytes(req_row.at[pl.ds(0, 7)], req_send)
        sent_bytes(req_row.at[pl.ds(0, 7)], req_send)

    def hand(slot, start, size):
        view = wo_buf.at[slot, pl.ds(base + start, size)]
        pltpu.make_async_remote_copy(
            src_ref=view,
            dst_ref=view,
            send_sem=d_send,
            recv_sem=d_recv,
            device_id=(z, y, 1 - c, t),
            device_id_type=MESH,
        ).start()

    def out_sides(i):
        with jax.named_scope("osides"):
            orr.wait_sides(i)
        orr.forward(i)
        for slot in (orr.left, orr.right):
            hand(slot, *outs[i])

    out_sides(0)

    def share(h, n):
        s = lax.rem(t + n, 4)
        cols = pl.ds(h * HD, HD)
        return pltpu.make_async_remote_copy(
            src_ref=att_buf.at[pl.ds(s * 128, 128), cols],
            dst_ref=attx.at[t, :, cols],
            send_sem=a_send,
            recv_sem=a_recv.at[h // 2, n],
            device_id=(z, y, c, s),
            device_id_type=MESH,
        )

    for unit in range(12):
        h, step = divmod(unit, 4)
        with jax.named_scope("ksent"):
            wait_sent_k(unit)
        if unit + AHEAD < 12:
            send_k(unit + AHEAD)
        if unit == 1:
            each_v(lambda n: slot_v(n, 1).start())
        if unit == 5:
            each_v(lambda n: slot_v(n, 2).start())
        if unit == 5:
            out_sides(1)

        @pl.when(step <= z)
        def _():
            g = z - step
            with jax.named_scope("wk"):
                sent_bytes(fark.at[g, h, pl.ds(0, 7)], ks_recv.at[g, h])
            with jax.named_scope("wv"):
                for core in range(2):

                    @pl.when(g * 2 + core != zc)
                    def _():
                        wait_v(g * 2 + core, h)

            with jax.named_scope("far"):
                bias = bias_far[g]
                s = score(fark[g, h].reshape(512, HD), h).reshape(16, 32, 512)
                s = (s + bias[:, None, :]).reshape(512, 512)
                absorb(h, s, farv[g, h].reshape(512, HD))

        if step == 3:
            with jax.named_scope("finish"):
                attended = acc_buf[h] / l_buf[h]
                att_buf[:, h * HD : (h + 1) * HD] = attended.T.astype(BF16)
                for n in (2, 1, 3):
                    share(h, n).start()

    with jax.named_scope("oopp"):
        for i in range(2):
            orr.wait_opp(i)
            hand(orr.opp, *outs[i])

    total = dot(att_buf[pl.ds(pl.multiple_of(t * 128, 128), 128), :], wo_buf[t])
    with jax.named_scope("handed"):
        sent_bytes(wo_buf.at[pl.ds(0, 3), pl.ds(0, 192)], d_recv)
    for n in (1, 3, 2):
        s = lax.rem(t + n, 4)
        with jax.named_scope("awaited"):
            sent_bytes(attx.at[s, :, pl.ds(0, 2 * HD)], a_recv.at[0, 4 - n])
        with jax.named_scope("outn"):
            total = total + dot(attx[s, :, 0 : 2 * HD], wo_buf[s, 0 : 2 * HD, :])
    for n in (1, 3, 2):
        s = lax.rem(t + n, 4)
        with jax.named_scope("awaited2"):
            sent_bytes(attx.at[s, :, pl.ds(2 * HD, HD)], a_recv.at[1, 4 - n])
        with jax.named_scope("outn2"):
            total = total + dot(attx[s, :, 2 * HD : 3 * HD], wo_buf[s, 2 * HD : 3 * HD, :])
    out_ref[...] = total.astype(BF16)

    with jax.named_scope("drain2"):
        orr.drain()
        sent_bytes(wo_buf.at[pl.ds(0, 3), pl.ds(0, 192)], d_send)
        sent_bytes(attx.at[pl.ds(0, 3)], a_send)
        each_v(lambda n: slot_v(n, 0).wait_send())
        each_v(lambda n: slot_v(n, 1).wait_send())
        each_v(lambda n: slot_v(n, 2).wait_send())


def local(tokens, w_query, w_key, w_value, w_out, chosen):
    any_ = pl.BlockSpec(memory_space=pltpu.HBM)
    vmem = pl.BlockSpec(memory_space=pltpu.VMEM)
    dma = pltpu.SemaphoreType.DMA
    return pl.pallas_call(
        body,
        out_shape=jax.ShapeDtypeStruct((128, 2048), BF16),
        in_specs=[any_] * 5 + [vmem],
        out_specs=vmem,
        scratch_shapes=[
            pltpu.VMEM((4, 512, 512), BF16),
            pltpu.VMEM((4, 512, 1152), BF16),
            pltpu.VMEM((512, 384), BF16),
            pltpu.VMEM((4, 16, 32, 384), BF16),
            pltpu.VMEM((4, 16, 32, 384), BF16),
            pltpu.VMEM((4, 384, 2048), BF16),
            pltpu.VMEM((4, 3, 8, 64, HD), BF16),
            pltpu.VMEM((8, 3, 4, 64, HD), BF16),
            pltpu.VMEM((4, 3, 8, 64, HD), BF16),
            pltpu.VMEM((4, 3, 4, 2, 64, HD), BF16),
            pltpu.VMEM((512, 384), BF16),
            pltpu.VMEM((4, 128, 384), BF16),
            pltpu.VMEM((512, 512), F32),
            pltpu.VMEM((5, 16, 512), F32),
            pltpu.VMEM((3, 1, 512), F32),
            pltpu.VMEM((3, 1, 512), F32),
            pltpu.VMEM((3, 128, 512), F32),
            pltpu.VMEM((8, 8, 512), jnp.int32),
            pltpu.VMEM((8, 8, 512), jnp.int32),
            pltpu.SMEM((8, 512), jnp.int32),
            pltpu.SMEM((8, 512), jnp.int32),
            dma((7,)),
            dma,
            dma((2,)),
            dma, dma((4, CHUNKS)), dma, dma((4, CHUNKS)),
            dma, dma((4, CHUNKS)), dma, dma((4, 2)),
            dma((12,)), dma((4, 3)), dma((3, 8)), dma((3, 8)),
            dma, dma, dma, dma((2, 4)),
        ],
        compiler_params=pltpu.CompilerParams(
            collective_id=0, has_side_effects=True, vmem_limit_bytes=56_000_000
        ),
        name="layer",
    )(
        tokens,
        w_query.reshape(4, 512, 384),
        w_key.reshape(4, 512, 384),
        w_value.reshape(4, 512, 384),
        w_out,
        chosen,
    )


def solution(mesh):
    finer = Mesh(mesh.devices.reshape(4, 4, 2, mesh.shape["tp"]), KV_TP)
    placed = (P(KV, "tp"), P(None, "tp"), P(None, "tp"), P(None, "tp"), P("tp", None), P(KV, None))
    return jax.shard_map(
        local, mesh=finer, in_specs=placed, out_specs=P(KV_TP, None), check_vma=False
    )
```

```python
import functools
import math

import jax
import jax.numpy as jnp
from jax import lax
from jax.experimental import pallas as pl
from jax.experimental.pallas import tpu as pltpu
from jax.sharding import Mesh
from jax.sharding import PartitionSpec as P

HD = 128
BLK = 32
SEL = 24
KV = ("kv_0", "kv_1", "kv_2")
KV_TP = ("kv_0", "kv_1", "kv_2", "tp")
NEG = -1e30
MESH = pl.DeviceIdType.MESH
F32 = jnp.float32
BF16 = jnp.bfloat16
SIZES = (3, 4, 4, 3, 2)
STARTS = (0, 3, 7, 11, 14)
CHUNKS = len(SIZES)
PASSED = 4
AHEAD = 5
LOG2E = 1.4426950408889634


def dot(a, b):
    return jnp.dot(a, b, preferred_element_type=F32)


def dot_t(a, b):
    return lax.dot_general(a, b, (((1,), (1,)), ((), ())), preferred_element_type=F32)


def dot_0(a, b):
    return lax.dot_general(a, b, (((0,), (0,)), ((), ())), preferred_element_type=F32)


def sent_bytes(view, sem):
    pltpu.make_async_copy(view, view, sem).wait()


class Ring:
    def __init__(self, buf, axis, chunks, coords, sems, grain=1):
        self.buf, self.axis, self.chunks, self.grain = buf, axis, chunks, grain
        self.me = coords[axis]
        self.right = lax.rem(self.me + 1, 4)
        self.left = lax.rem(self.me + 3, 4)
        self.opp = lax.rem(self.me + 2, 4)
        self.coords = coords
        self.send, self.recv = sems

    def _copy(self, slot, start, size, target, kind, i):
        view = self.buf.at[slot, pl.ds(start, size)]
        return pltpu.make_async_remote_copy(
            src_ref=view,
            dst_ref=view,
            send_sem=self.send,
            recv_sem=self.recv.at[kind, i],
            device_id=tuple(target if a == self.axis else self.coords[a] for a in KV_TP),
            device_id_type=MESH,
        )

    def _start(self, *args):
        self._copy(*args).start()

    def start_own(self, i):
        start, size = self.chunks[i]
        self._start(self.me, start, size, self.right, 0, i)
        self._start(self.me, start, size, self.left, 1, i)

    def wait_sides(self, i):
        start, size = self.chunks[i]
        self._copy(self.left, start, size, self.right, 0, i).wait_recv()
        self._copy(self.right, start, size, self.left, 1, i).wait_recv()

    def half(self, size):
        return -(-size // (2 * self.grain)) * self.grain

    def forward(self, i):
        start, size = self.chunks[i]
        half = self.half(size)
        self._start(self.left, start, half, self.right, 2, i)
        self._start(self.right, start + half, size - half, self.left, 3, i)

    def start_all(self, i):
        self.start_own(i)
        self._start(self.me, *self.chunks[i], self.opp, 2, i)

    def wait_all(self, i):
        self.wait_sides(i)
        self._copy(self.opp, *self.chunks[i], self.opp, 2, i).wait_recv()

    def wait_opp(self, i):
        start, size = self.chunks[i]
        half = self.half(size)
        self._copy(self.opp, start, half, self.right, 2, i).wait_recv()
        self._copy(self.opp, start + half, size - half, self.left, 3, i).wait_recv()

    def drain(self):
        start = self.chunks[0][0]
        size = sum(n for _, n in self.chunks)
        sent_bytes(self.buf.at[pl.ds(0, 3), pl.ds(start, size)], self.send)


def body(
    tok_hbm, wq_hbm, wk_hbm, wv_hbm, wo_hbm, chosen_ref,
    out_ref,
    x_buf, w_buf, q_buf, k_buf, v_buf, wo_buf,
    stk, stv, fark, farv, att_buf, attx,
    bias_own, bias_far, m_buf, l_buf, acc_buf,
    req_row, req_col, smem_row, smem_col,
    local_sem, req_send, req_recv,
    x_send, x_recv, k_send, k_recv, v_send, v_recv, o_send, o_recv,
    ks_send, ks_recv, vs_send, vs_recv, d_send, d_recv, a_send, a_recv,
):
    z, y, c, t = (lax.axis_index(a) for a in KV_TP)
    coords = dict(zip(KV_TP, (z, y, c, t)))
    me = z * 8 + y * 2 + c
    yc = y * 2 + c
    zc = z * 2 + c

    locals_ = [pltpu.make_async_copy(tok_hbm, x_buf.at[t], local_sem.at[0])]
    for n, w in enumerate((wq_hbm, wk_hbm, wv_hbm)):
        locals_.append(
            pltpu.make_async_copy(w, w_buf.at[:, :, pl.ds(n * 384, 384)], local_sem.at[1 + n])
        )
    locals_.append(pltpu.make_async_copy(wo_hbm, wo_buf.at[t], local_sem.at[4]))
    for copy in locals_:
        copy.start()

    def row_peer(n):
        j = lax.rem(yc + n, 8)
        return j, (z, j // 2, lax.rem(j, 2), t)

    def col_peer(n):
        j = lax.rem(zc + n, 8)
        return j, (j // 2, y, lax.rem(j, 2), t)

    barrier = pltpu.get_barrier_semaphore()
    for n in range(1, 4):
        pl.semaphore_signal(
            barrier, inc=1, device_id=(z, y, c, lax.rem(t + n, 4)), device_id_type=MESH
        )
    for n in range(1, 8):
        pl.semaphore_signal(barrier, inc=1, device_id=row_peer(n)[1], device_id_type=MESH)
    for n in range(1, 8):
        pl.semaphore_signal(barrier, inc=1, device_id=col_peer(n)[1], device_id_type=MESH)
    with jax.named_scope("barrier"):
        pl.semaphore_wait(barrier, 17)

    blocks = tuple(zip(STARTS, SIZES))
    xr = Ring(
        x_buf, "tp", tuple((p * BLK, n * BLK) for p, n in blocks), coords, (x_send, x_recv)
    )
    kr = Ring(k_buf, "kv_0", blocks, coords, (k_send, k_recv))
    vr = Ring(v_buf, "kv_1", blocks, coords, (v_send, v_recv))
    base = c * 192
    outs = ((0, 96), (96, 96))
    orr = Ring(
        wo_buf, "tp", tuple((base + p, n) for p, n in outs), coords, (o_send, o_recv), grain=16
    )

    locals_[0].wait()
    xr.start_own(0)
    xr.start_own(1)

    with jax.named_scope("plan"):
        chosen = chosen_ref[...]
        lane = lax.broadcasted_iota(jnp.int32, (16, 512), 1)
        sub = lax.broadcasted_iota(jnp.int32, (16, 512), 0)
        hit_all = jnp.zeros((16, 512), jnp.bool_)
        for e in range(SEL):
            hit_all = hit_all | (chosen[:, e : e + 1] == lane)
        lane8 = lax.broadcasted_iota(jnp.int32, (8, 512), 1)
        wanted = jnp.max(jnp.where(hit_all & (lane // 16 != me), 1, 0), axis=0, keepdims=True)
        wanted = jnp.broadcast_to(wanted, (8, 512))
        place = lane8 % 16

        def scan(value):
            for step in (1, 2, 4, 8):
                value = value + jnp.where(place >= step, pltpu.roll(value, step, 1), 0)
            return value

        count = scan(wanted)
        first = scan(jnp.where((wanted == 1) & (count == 1), place + 1, 0))
        second = scan(jnp.where((wanted == 1) & (count == 2), place + 1, 0))
        asked = jnp.where(
            place == 15, first, jnp.where(place == 14, pltpu.roll(second, 511, 1), 0)
        )
        row = jnp.maximum(asked - 1, 0)
        req_row[pl.ds(yc, 1)] = row.reshape(1, 8, 512)
        req_col[pl.ds(zc, 1)] = row.reshape(1, 8, 512)

    for n in range(1, 8):
        for which, buf, mine, peer in ((0, req_row, yc, row_peer), (1, req_col, zc, col_peer)):
            copy = pltpu.make_async_remote_copy(
                src_ref=buf.at[mine],
                dst_ref=buf.at[mine],
                send_sem=req_send,
                recv_sem=req_recv.at[which],
                device_id=peer(n)[1],
                device_id_type=MESH,
            )
            copy.start()

    with jax.named_scope("masks"):
        widen = jnp.where(sub == lane // 32, 1.0, 0.0).astype(BF16)
        high = dot_0((chosen // 16).astype(F32).astype(BF16), widen)
        low = dot_0((chosen % 16).astype(F32).astype(BF16), widen)
        chosen_t = high.astype(jnp.int32) * 16 + low.astype(jnp.int32)
        asked_f = asked.astype(F32).astype(BF16)
        for g in range(5):
            if g < 4:
                spread = jnp.where(lane == (g * 8 + sub // 2) * 16 + 15 - sub % 2, 1.0, 0.0)
                value = dot_t(spread.astype(BF16), asked_f).astype(jnp.int32)[:, 0:1]
                sub1 = sub[:, 0:1]
                ids = jnp.where(value > 0, (g * 8 + sub1 // 2) * 16 + value - 1, -1)
                ids = jnp.broadcast_to(ids, (16, 512))
            else:
                ids = me * 16 + sub
            hit = jnp.zeros((16, 512), jnp.bool_)
            for e in range(SEL):
                hit = hit | (chosen_t[e : e + 1, :] == ids)
            bias_far[g] = jnp.where(hit, 0.0, NEG)
        ti = lax.broadcasted_iota(jnp.int32, (512, 512), 0)
        tj = lax.broadcasted_iota(jnp.int32, (512, 512), 1)
        seen = jnp.broadcast_to(bias_far[4][:, None, :], (16, 32, 512)).reshape(512, 512)
        bias_own[...] = jnp.where(ti <= tj, seen, NEG)
        m_buf[...] = jnp.full(m_buf.shape, NEG, F32)
        l_buf[...] = jnp.zeros(l_buf.shape, F32)
        acc_buf[...] = jnp.zeros(acc_buf.shape, F32)

    for copy in locals_[1:4]:
        copy.wait()

    def next_sides(i):
        with jax.named_scope("xsides"):
            xr.wait_sides(i)
        xr.forward(i)
        if i + 2 < CHUNKS:
            xr.start_own(i + 2)

    next_sides(0)
    for i in range(CHUNKS):
        first, size = blocks[i]
        rows = slice(first * BLK, (first + size) * BLK)
        if i >= 1:
            for ring in (kr, vr):
                (ring.start_own if i - 1 < PASSED else ring.start_all)(i - 1)
        acc = dot(x_buf[t, rows, :], w_buf[t])
        acc = acc + dot(x_buf[xr.left, rows, :], w_buf[xr.left])
        acc = acc + dot(x_buf[xr.right, rows, :], w_buf[xr.right])
        if i + 1 < CHUNKS:
            next_sides(i + 1)
        if i + 2 == CHUNKS:
            locals_[4].wait()
            orr.start_own(0)
        if i == 0:
            sent_bytes(req_row.at[pl.ds(0, 7)], req_recv.at[0])
            sent_bytes(req_col.at[pl.ds(0, 7)], req_recv.at[1])
            to_smem = [
                pltpu.make_async_copy(req_row.at[:, 0], smem_row, local_sem.at[5]),
                pltpu.make_async_copy(req_col.at[:, 0], smem_col, local_sem.at[6]),
            ]
            for copy in to_smem:
                copy.start()
        if i == 1:
            for copy in to_smem:
                copy.wait()
        if 0 <= i - 2 < PASSED:
            with jax.named_scope("kvsides"):
                for ring in (kr, vr):
                    ring.wait_sides(i - 2)
                    ring.forward(i - 2)
        with jax.named_scope("xopp"):
            xr.wait_opp(i)
        acc = acc + dot(x_buf[xr.opp, rows, :], w_buf[xr.opp])
        q_buf[rows, :] = (acc[:, 0:384] * (HD**-0.5 * LOG2E)).astype(BF16)
        k_buf[pl.ds(z, 1), first : first + size] = (
            acc[:, 384:768].astype(BF16).reshape(1, size, BLK, 384)
        )
        v_buf[pl.ds(y, 1), first : first + size] = (
            acc[:, 768:1152].astype(BF16).reshape(1, size, BLK, 384)
        )
    for ring in (kr, vr):
        ring.start_all(CHUNKS - 1)
    orr.start_own(1)
    for i in (3,):
        for ring in (kr, vr):
            ring.wait_sides(i)
            ring.forward(i)
    with jax.named_scope("kvopp"):
        for i in range(CHUNKS):
            for ring in (kr, vr):
                (ring.wait_opp if i < PASSED else ring.wait_all)(i)

    def score(k, h):
        return dot_t(k, q_buf[:, h * HD : (h + 1) * HD])

    def absorb(h, s, v):
        m_old = m_buf[h]
        m_new = jnp.maximum(m_old, jnp.max(s, axis=0, keepdims=True))
        p = jnp.exp2(s - m_new)
        scale = jnp.exp2(m_old - m_new)
        m_buf[h] = m_new
        l_buf[h] = l_buf[h] * scale + jnp.sum(p, axis=0, keepdims=True)
        acc_buf[h] = acc_buf[h] * scale + dot_0(v, p.astype(BF16))

    def slot_k(n, unit):
        h, step = divmod(unit, 4)
        j, device = row_peer(n)
        return pltpu.make_async_remote_copy(
            src_ref=stk.at[z - step, h, j],
            dst_ref=fark.at[z - step, h, yc],
            send_sem=ks_send.at[unit],
            recv_sem=ks_recv.at[z - step, h],
            device_id=device,
            device_id_type=MESH,
        )

    def send_k(unit):
        @pl.when(unit % 4 <= z)
        def _():
            for n in order:
                slot_k(n, unit).start()

    def wait_sent_k(unit):
        @pl.when(unit % 4 <= z)
        def _():
            sent_bytes(stk.at[0, 0, pl.ds(0, 7)], ks_send.at[unit])

    def slot_v(n, h):
        j, device = col_peer(n)
        return pltpu.make_async_remote_copy(
            src_ref=stv.at[j, h],
            dst_ref=farv.at[z, h, :, c],
            send_sem=vs_send.at[h, n],
            recv_sem=vs_recv.at[h, n],
            device_id=device,
            device_id_type=MESH,
        )

    def each_v(action):
        for n in (1, 2, 3, 6, 7, 4, 5):

            @pl.when(col_peer(n)[0] // 2 >= z)
            def _():
                action(n)

    def wait_v(j, h):
        n = lax.rem(zc - j + 8, 8)
        pltpu.make_async_remote_copy(
            src_ref=stv.at[j, h],
            dst_ref=farv.at[j // 2, h, :, lax.rem(j, 2)],
            send_sem=vs_send.at[h, n],
            recv_sem=vs_recv.at[h, n],
            device_id=(j // 2, y, lax.rem(j, 2), t),
            device_id_type=MESH,
        ).wait_recv()

    def stage_v(j, carry):
        for s in range(4):
            for k in range(2):
                b = smem_col[j, (z * 8 + s * 2 + c) * 16 + 15 - k]
                block = v_buf[s, b]
                for h in range(3):
                    stv[j, h, s, pl.ds(k * BLK, BLK), :] = block[:, h * HD : (h + 1) * HD]
        return carry

    def stage_k(j, carry):
        for g in range(4):
            for k in range(2):
                b = smem_row[j, (g * 8 + yc) * 16 + 15 - k]
                block = k_buf[g, b]
                for h in range(3):
                    stk[g, h, j, pl.ds(k * BLK, BLK), :] = block[:, h * HD : (h + 1) * HD]
        return carry

    order = (4, 5, 3, 2, 6, 7, 1)
    with jax.named_scope("stage"):
        lax.fori_loop(0, 8, stage_k, 0)
        lax.fori_loop(0, 8, stage_v, 0)
    with jax.named_scope("sends"):
        send_k(0)
        each_v(lambda n: slot_v(n, 0).start())
        send_k(1)
        for unit in range(2, AHEAD):
            send_k(unit)
    for h in range(3):
        for g in range(4):
            fark[g, h, pl.ds(yc, 1)] = stk[g, h, pl.ds(yc, 1)]
        for s in range(4):
            farv[pl.ds(z, 1), h, s, pl.ds(c, 1)] = stv[pl.ds(zc, 1), h, s].reshape(1, 1, 64, HD)

    with jax.named_scope("own"):
        k_own = k_buf[z].reshape(512, 384)
        v_own = v_buf[y].reshape(512, 384)
        later = score(k_own[:, 0:HD], 0)
        for h in range(3):
            s = later + bias_own[...]
            if h < 2:
                later = score(k_own[:, (h + 1) * HD : (h + 2) * HD], h + 1)
            absorb(h, s, v_own[:, h * HD : (h + 1) * HD])
    with jax.named_scope("drain1"):
        for ring in (xr, kr, vr):
            ring.drain()
        sent_bytes(req_row.at[pl.ds(0, 7)], req_send)
        sent_bytes(req_row.at[pl.ds(0, 7)], req_send)

    def hand(slot, start, size):
        view = wo_buf.at[slot, pl.ds(base + start, size)]
        pltpu.make_async_remote_copy(
            src_ref=view,
            dst_ref=view,
            send_sem=d_send,
            recv_sem=d_recv,
            device_id=(z, y, 1 - c, t),
            device_id_type=MESH,
        ).start()

    def out_sides(i):
        with jax.named_scope("osides"):
            orr.wait_sides(i)
        orr.forward(i)
        for slot in (orr.left, orr.right):
            hand(slot, *outs[i])

    out_sides(0)

    def share(h, n):
        s = lax.rem(t + n, 4)
        cols = pl.ds(h * HD, HD)
        return pltpu.make_async_remote_copy(
            src_ref=att_buf.at[pl.ds(s * 128, 128), cols],
            dst_ref=attx.at[t, :, cols],
            send_sem=a_send,
            recv_sem=a_recv.at[h // 2, n],
            device_id=(z, y, c, s),
            device_id_type=MESH,
        )

    for unit in range(12):
        h, step = divmod(unit, 4)
        with jax.named_scope("ksent"):
            wait_sent_k(unit)
        if unit + AHEAD < 12:
            send_k(unit + AHEAD)
        if unit == 1:
            each_v(lambda n: slot_v(n, 1).start())
        if unit == 5:
            each_v(lambda n: slot_v(n, 2).start())
        if unit == 3:
            out_sides(1)

        @pl.when(step <= z)
        def _():
            g = z - step
            with jax.named_scope("wk"):
                sent_bytes(fark.at[g, h, pl.ds(0, 7)], ks_recv.at[g, h])
            with jax.named_scope("wv"):
                for core in range(2):

                    @pl.when(g * 2 + core != zc)
                    def _():
                        wait_v(g * 2 + core, h)

            with jax.named_scope("far"):
                bias = bias_far[g]
                s = score(fark[g, h].reshape(512, HD), h).reshape(16, 32, 512)
                s = (s + bias[:, None, :]).reshape(512, 512)
                absorb(h, s, farv[g, h].reshape(512, HD))

        if step == 3:
            with jax.named_scope("finish"):
                attended = acc_buf[h] / l_buf[h]
                att_buf[:, h * HD : (h + 1) * HD] = attended.T.astype(BF16)
                for n in (2, 1, 3):
                    share(h, n).start()

    with jax.named_scope("oopp"):
        for i in range(2):
            orr.wait_opp(i)
            hand(orr.opp, *outs[i])

    total = dot(att_buf[pl.ds(pl.multiple_of(t * 128, 128), 128), :], wo_buf[t])
    with jax.named_scope("handed"):
        sent_bytes(wo_buf.at[pl.ds(0, 3), pl.ds(0, 192)], d_recv)
    for n in (1, 3, 2):
        s = lax.rem(t + n, 4)
        with jax.named_scope("awaited"):
            sent_bytes(attx.at[s, :, pl.ds(0, 2 * HD)], a_recv.at[0, 4 - n])
        with jax.named_scope("outn"):
            total = total + dot(attx[s, :, 0 : 2 * HD], wo_buf[s, 0 : 2 * HD, :])
    for n in (1, 3, 2):
        s = lax.rem(t + n, 4)
        with jax.named_scope("awaited2"):
            sent_bytes(attx.at[s, :, pl.ds(2 * HD, HD)], a_recv.at[1, 4 - n])
        with jax.named_scope("outn2"):
            total = total + dot(attx[s, :, 2 * HD : 3 * HD], wo_buf[s, 2 * HD : 3 * HD, :])
    out_ref[...] = total.astype(BF16)

    with jax.named_scope("drain2"):
        orr.drain()
        sent_bytes(wo_buf.at[pl.ds(0, 3), pl.ds(0, 192)], d_send)
        sent_bytes(attx.at[pl.ds(0, 3)], a_send)
        each_v(lambda n: slot_v(n, 0).wait_send())
        each_v(lambda n: slot_v(n, 1).wait_send())
        each_v(lambda n: slot_v(n, 2).wait_send())


def local(tokens, w_query, w_key, w_value, w_out, chosen):
    any_ = pl.BlockSpec(memory_space=pltpu.HBM)
    vmem = pl.BlockSpec(memory_space=pltpu.VMEM)
    dma = pltpu.SemaphoreType.DMA
    return pl.pallas_call(
        body,
        out_shape=jax.ShapeDtypeStruct((128, 2048), BF16),
        in_specs=[any_] * 5 + [vmem],
        out_specs=vmem,
        scratch_shapes=[
            pltpu.VMEM((4, 512, 512), BF16),
            pltpu.VMEM((4, 512, 1152), BF16),
            pltpu.VMEM((512, 384), BF16),
            pltpu.VMEM((4, 16, 32, 384), BF16),
            pltpu.VMEM((4, 16, 32, 384), BF16),
            pltpu.VMEM((4, 384, 2048), BF16),
            pltpu.VMEM((4, 3, 8, 64, HD), BF16),
            pltpu.VMEM((8, 3, 4, 64, HD), BF16),
            pltpu.VMEM((4, 3, 8, 64, HD), BF16),
            pltpu.VMEM((4, 3, 4, 2, 64, HD), BF16),
            pltpu.VMEM((512, 384), BF16),
            pltpu.VMEM((4, 128, 384), BF16),
            pltpu.VMEM((512, 512), F32),
            pltpu.VMEM((5, 16, 512), F32),
            pltpu.VMEM((3, 1, 512), F32),
            pltpu.VMEM((3, 1, 512), F32),
            pltpu.VMEM((3, 128, 512), F32),
            pltpu.VMEM((8, 8, 512), jnp.int32),
            pltpu.VMEM((8, 8, 512), jnp.int32),
            pltpu.SMEM((8, 512), jnp.int32),
            pltpu.SMEM((8, 512), jnp.int32),
            dma((7,)),
            dma,
            dma((2,)),
            dma, dma((4, CHUNKS)), dma, dma((4, CHUNKS)),
            dma, dma((4, CHUNKS)), dma, dma((4, 2)),
            dma((12,)), dma((4, 3)), dma((3, 8)), dma((3, 8)),
            dma, dma, dma, dma((2, 4)),
        ],
        compiler_params=pltpu.CompilerParams(
            collective_id=0, has_side_effects=True, vmem_limit_bytes=56_000_000
        ),
        name="layer",
    )(
        tokens,
        w_query.reshape(4, 512, 384),
        w_key.reshape(4, 512, 384),
        w_value.reshape(4, 512, 384),
        w_out,
        chosen,
    )


def solution(mesh):
    finer = Mesh(mesh.devices.reshape(4, 4, 2, mesh.shape["tp"]), KV_TP)
    placed = (P(KV, "tp"), P(None, "tp"), P(None, "tp"), P(None, "tp"), P("tp", None), P(KV, None))
    return jax.shard_map(
        local, mesh=finer, in_specs=placed, out_specs=P(KV_TP, None), check_vma=False
    )
```

```python
import functools
import math

import jax
import jax.numpy as jnp
from jax import lax
from jax.experimental import pallas as pl
from jax.experimental.pallas import tpu as pltpu
from jax.sharding import Mesh
from jax.sharding import PartitionSpec as P

HD = 128
BLK = 32
SEL = 24
KV = ("kv_0", "kv_1", "kv_2")
KV_TP = ("kv_0", "kv_1", "kv_2", "tp")
NEG = -1e30
MESH = pl.DeviceIdType.MESH
F32 = jnp.float32
BF16 = jnp.bfloat16
SIZES = (3, 4, 4, 3, 2)
STARTS = (0, 3, 7, 11, 14)
CHUNKS = len(SIZES)
PASSED = 4
AHEAD = 5
LOG2E = 1.4426950408889634


def dot(a, b):
    return jnp.dot(a, b, preferred_element_type=F32)


def dot_t(a, b):
    return lax.dot_general(a, b, (((1,), (1,)), ((), ())), preferred_element_type=F32)


def dot_0(a, b):
    return lax.dot_general(a, b, (((0,), (0,)), ((), ())), preferred_element_type=F32)


def sent_bytes(view, sem):
    pltpu.make_async_copy(view, view, sem).wait()


class Ring:
    def __init__(self, buf, axis, chunks, coords, sems, grain=1):
        self.buf, self.axis, self.chunks, self.grain = buf, axis, chunks, grain
        self.me = coords[axis]
        self.right = lax.rem(self.me + 1, 4)
        self.left = lax.rem(self.me + 3, 4)
        self.opp = lax.rem(self.me + 2, 4)
        self.coords = coords
        self.send, self.recv = sems

    def _copy(self, slot, start, size, target, kind, i):
        view = self.buf.at[slot, pl.ds(start, size)]
        return pltpu.make_async_remote_copy(
            src_ref=view,
            dst_ref=view,
            send_sem=self.send,
            recv_sem=self.recv.at[kind, i],
            device_id=tuple(target if a == self.axis else self.coords[a] for a in KV_TP),
            device_id_type=MESH,
        )

    def _start(self, *args):
        self._copy(*args).start()

    def start_own(self, i):
        start, size = self.chunks[i]
        self._start(self.me, start, size, self.right, 0, i)
        self._start(self.me, start, size, self.left, 1, i)

    def wait_sides(self, i):
        start, size = self.chunks[i]
        self._copy(self.left, start, size, self.right, 0, i).wait_recv()
        self._copy(self.right, start, size, self.left, 1, i).wait_recv()

    def half(self, size):
        return -(-size // (2 * self.grain)) * self.grain

    def forward(self, i):
        start, size = self.chunks[i]
        half = self.half(size)
        self._start(self.left, start, half, self.right, 2, i)
        self._start(self.right, start + half, size - half, self.left, 3, i)

    def start_all(self, i):
        self.start_own(i)
        self._start(self.me, *self.chunks[i], self.opp, 2, i)

    def wait_all(self, i):
        self.wait_sides(i)
        self._copy(self.opp, *self.chunks[i], self.opp, 2, i).wait_recv()

    def wait_opp(self, i):
        start, size = self.chunks[i]
        half = self.half(size)
        self._copy(self.opp, start, half, self.right, 2, i).wait_recv()
        self._copy(self.opp, start + half, size - half, self.left, 3, i).wait_recv()

    def drain(self):
        start = self.chunks[0][0]
        size = sum(n for _, n in self.chunks)
        sent_bytes(self.buf.at[pl.ds(0, 3), pl.ds(start, size)], self.send)


def body(
    tok_hbm, wq_hbm, wk_hbm, wv_hbm, wo_hbm, chosen_ref,
    out_ref,
    x_buf, w_buf, q_buf, k_buf, v_buf, wo_buf,
    stk, stv, fark, farv, att_buf, attx,
    bias_own, bias_far, m_buf, l_buf, acc_buf,
    req_row, req_col, smem_row, smem_col,
    local_sem, req_send, req_recv,
    x_send, x_recv, k_send, k_recv, v_send, v_recv, o_send, o_recv,
    ks_send, ks_recv, vs_send, vs_recv, d_send, d_recv, a_send, a_recv,
):
    z, y, c, t = (lax.axis_index(a) for a in KV_TP)
    coords = dict(zip(KV_TP, (z, y, c, t)))
    me = z * 8 + y * 2 + c
    yc = y * 2 + c
    zc = z * 2 + c

    locals_ = [pltpu.make_async_copy(tok_hbm, x_buf.at[t], local_sem.at[0])]
    for n, w in enumerate((wq_hbm, wk_hbm, wv_hbm)):
        locals_.append(
            pltpu.make_async_copy(w, w_buf.at[:, :, pl.ds(n * 384, 384)], local_sem.at[1 + n])
        )
    locals_.append(pltpu.make_async_copy(wo_hbm, wo_buf.at[t], local_sem.at[4]))
    for copy in locals_:
        copy.start()

    def row_peer(n):
        j = lax.rem(yc + n, 8)
        return j, (z, j // 2, lax.rem(j, 2), t)

    def col_peer(n):
        j = lax.rem(zc + n, 8)
        return j, (j // 2, y, lax.rem(j, 2), t)

    barrier = pltpu.get_barrier_semaphore()
    for n in range(1, 4):
        pl.semaphore_signal(
            barrier, inc=1, device_id=(z, y, c, lax.rem(t + n, 4)), device_id_type=MESH
        )
    for n in range(1, 8):
        pl.semaphore_signal(barrier, inc=1, device_id=row_peer(n)[1], device_id_type=MESH)
    for n in range(1, 8):
        pl.semaphore_signal(barrier, inc=1, device_id=col_peer(n)[1], device_id_type=MESH)
    with jax.named_scope("barrier"):
        pl.semaphore_wait(barrier, 17)

    blocks = tuple(zip(STARTS, SIZES))
    xr = Ring(
        x_buf, "tp", tuple((p * BLK, n * BLK) for p, n in blocks), coords, (x_send, x_recv)
    )
    kr = Ring(k_buf, "kv_0", blocks, coords, (k_send, k_recv))
    vr = Ring(v_buf, "kv_1", blocks, coords, (v_send, v_recv))
    base = c * 192
    outs = ((0, 96), (96, 96))
    orr = Ring(
        wo_buf, "tp", tuple((base + p, n) for p, n in outs), coords, (o_send, o_recv), grain=16
    )

    locals_[0].wait()
    xr.start_own(0)
    xr.start_own(1)

    with jax.named_scope("plan"):
        chosen = chosen_ref[...]
        lane = lax.broadcasted_iota(jnp.int32, (16, 512), 1)
        sub = lax.broadcasted_iota(jnp.int32, (16, 512), 0)
        hit_all = jnp.zeros((16, 512), jnp.bool_)
        for e in range(SEL):
            hit_all = hit_all | (chosen[:, e : e + 1] == lane)
        lane8 = lax.broadcasted_iota(jnp.int32, (8, 512), 1)
        wanted = jnp.max(jnp.where(hit_all & (lane // 16 != me), 1, 0), axis=0, keepdims=True)
        wanted = jnp.broadcast_to(wanted, (8, 512))
        place = lane8 % 16

        def scan(value):
            for step in (1, 2, 4, 8):
                value = value + jnp.where(place >= step, pltpu.roll(value, step, 1), 0)
            return value

        count = scan(wanted)
        first = scan(jnp.where((wanted == 1) & (count == 1), place + 1, 0))
        second = scan(jnp.where((wanted == 1) & (count == 2), place + 1, 0))
        asked = jnp.where(
            place == 15, first, jnp.where(place == 14, pltpu.roll(second, 511, 1), 0)
        )
        row = jnp.maximum(asked - 1, 0)
        req_row[pl.ds(yc, 1)] = row.reshape(1, 8, 512)
        req_col[pl.ds(zc, 1)] = row.reshape(1, 8, 512)

    for n in range(1, 8):
        for which, buf, mine, peer in ((0, req_row, yc, row_peer), (1, req_col, zc, col_peer)):
            copy = pltpu.make_async_remote_copy(
                src_ref=buf.at[mine],
                dst_ref=buf.at[mine],
                send_sem=req_send,
                recv_sem=req_recv.at[which],
                device_id=peer(n)[1],
                device_id_type=MESH,
            )
            copy.start()

    with jax.named_scope("masks"):
        widen = jnp.where(sub == lane // 32, 1.0, 0.0).astype(BF16)
        high = dot_0((chosen // 16).astype(F32).astype(BF16), widen)
        low = dot_0((chosen % 16).astype(F32).astype(BF16), widen)
        chosen_t = high.astype(jnp.int32) * 16 + low.astype(jnp.int32)
        asked_f = asked.astype(F32).astype(BF16)
        for g in range(5):
            if g < 4:
                spread = jnp.where(lane == (g * 8 + sub // 2) * 16 + 15 - sub % 2, 1.0, 0.0)
                value = dot_t(spread.astype(BF16), asked_f).astype(jnp.int32)[:, 0:1]
                sub1 = sub[:, 0:1]
                ids = jnp.where(value > 0, (g * 8 + sub1 // 2) * 16 + value - 1, -1)
                ids = jnp.broadcast_to(ids, (16, 512))
            else:
                ids = me * 16 + sub
            hit = jnp.zeros((16, 512), jnp.bool_)
            for e in range(SEL):
                hit = hit | (chosen_t[e : e + 1, :] == ids)
            bias_far[g] = jnp.where(hit, 0.0, NEG)
        ti = lax.broadcasted_iota(jnp.int32, (512, 512), 0)
        tj = lax.broadcasted_iota(jnp.int32, (512, 512), 1)
        seen = jnp.broadcast_to(bias_far[4][:, None, :], (16, 32, 512)).reshape(512, 512)
        bias_own[...] = jnp.where(ti <= tj, seen, NEG)
        m_buf[...] = jnp.full(m_buf.shape, NEG, F32)
        l_buf[...] = jnp.zeros(l_buf.shape, F32)
        acc_buf[...] = jnp.zeros(acc_buf.shape, F32)

    for copy in locals_[1:4]:
        copy.wait()

    def next_sides(i):
        with jax.named_scope("xsides"):
            xr.wait_sides(i)
        xr.forward(i)
        if i + 2 < CHUNKS:
            xr.start_own(i + 2)

    next_sides(0)
    for i in range(CHUNKS):
        first, size = blocks[i]
        rows = slice(first * BLK, (first + size) * BLK)
        if i >= 1:
            for ring in (kr, vr):
                (ring.start_own if i - 1 < PASSED else ring.start_all)(i - 1)
        acc = dot(x_buf[t, rows, :], w_buf[t])
        acc = acc + dot(x_buf[xr.left, rows, :], w_buf[xr.left])
        acc = acc + dot(x_buf[xr.right, rows, :], w_buf[xr.right])
        if i + 1 < CHUNKS:
            next_sides(i + 1)
        if i + 2 == CHUNKS:
            locals_[4].wait()
            orr.start_own(0)
        if i == 0:
            sent_bytes(req_row.at[pl.ds(0, 7)], req_recv.at[0])
            sent_bytes(req_col.at[pl.ds(0, 7)], req_recv.at[1])
            to_smem = [
                pltpu.make_async_copy(req_row.at[:, 0], smem_row, local_sem.at[5]),
                pltpu.make_async_copy(req_col.at[:, 0], smem_col, local_sem.at[6]),
            ]
            for copy in to_smem:
                copy.start()
        if i == 1:
            for copy in to_smem:
                copy.wait()
        if 0 <= i - 2 < PASSED:
            with jax.named_scope("kvsides"):
                for ring in (kr, vr):
                    ring.wait_sides(i - 2)
                    ring.forward(i - 2)
        with jax.named_scope("xopp"):
            xr.wait_opp(i)
        acc = acc + dot(x_buf[xr.opp, rows, :], w_buf[xr.opp])
        q_buf[rows, :] = (acc[:, 0:384] * (HD**-0.5 * LOG2E)).astype(BF16)
        k_buf[pl.ds(z, 1), first : first + size] = (
            acc[:, 384:768].astype(BF16).reshape(1, size, BLK, 384)
        )
        v_buf[pl.ds(y, 1), first : first + size] = (
            acc[:, 768:1152].astype(BF16).reshape(1, size, BLK, 384)
        )
    for ring in (kr, vr):
        ring.start_all(CHUNKS - 1)
    orr.start_own(1)
    for i in (3,):
        for ring in (kr, vr):
            ring.wait_sides(i)
            ring.forward(i)
    def score(k, h):
        return dot_t(k, q_buf[:, h * HD : (h + 1) * HD])

    def absorb(h, s, v):
        m_old = m_buf[h]
        m_new = jnp.maximum(m_old, jnp.max(s, axis=0, keepdims=True))
        p = jnp.exp2(s - m_new)
        scale = jnp.exp2(m_old - m_new)
        m_buf[h] = m_new
        l_buf[h] = l_buf[h] * scale + jnp.sum(p, axis=0, keepdims=True)
        acc_buf[h] = acc_buf[h] * scale + dot_0(v, p.astype(BF16))

    with jax.named_scope("own"):
        k_own = k_buf[z].reshape(512, 384)
        v_own = v_buf[y].reshape(512, 384)
        later = score(k_own[:, 0:HD], 0)
        for h in range(3):
            s = later + bias_own[...]
            if h < 2:
                later = score(k_own[:, (h + 1) * HD : (h + 2) * HD], h + 1)
            absorb(h, s, v_own[:, h * HD : (h + 1) * HD])
    with jax.named_scope("kvopp"):
        for i in range(CHUNKS):
            for ring in (kr, vr):
                (ring.wait_opp if i < PASSED else ring.wait_all)(i)

    def slot_k(n, unit):
        h, step = divmod(unit, 4)
        j, device = row_peer(n)
        return pltpu.make_async_remote_copy(
            src_ref=stk.at[z - step, h, j],
            dst_ref=fark.at[z - step, h, yc],
            send_sem=ks_send.at[unit],
            recv_sem=ks_recv.at[z - step, h],
            device_id=device,
            device_id_type=MESH,
        )

    def send_k(unit):
        @pl.when(unit % 4 <= z)
        def _():
            for n in order:
                slot_k(n, unit).start()

    def wait_sent_k(unit):
        @pl.when(unit % 4 <= z)
        def _():
            sent_bytes(stk.at[0, 0, pl.ds(0, 7)], ks_send.at[unit])

    def slot_v(n, h):
        j, device = col_peer(n)
        return pltpu.make_async_remote_copy(
            src_ref=stv.at[j, h],
            dst_ref=farv.at[z, h, :, c],
            send_sem=vs_send.at[h, n],
            recv_sem=vs_recv.at[h, n],
            device_id=device,
            device_id_type=MESH,
        )

    def each_v(action):
        for n in (1, 2, 3, 6, 7, 4, 5):

            @pl.when(col_peer(n)[0] // 2 >= z)
            def _():
                action(n)

    def wait_v(j, h):
        n = lax.rem(zc - j + 8, 8)
        pltpu.make_async_remote_copy(
            src_ref=stv.at[j, h],
            dst_ref=farv.at[j // 2, h, :, lax.rem(j, 2)],
            send_sem=vs_send.at[h, n],
            recv_sem=vs_recv.at[h, n],
            device_id=(j // 2, y, lax.rem(j, 2), t),
            device_id_type=MESH,
        ).wait_recv()

    def stage_v(j, carry):
        for s in range(4):
            for k in range(2):
                b = smem_col[j, (z * 8 + s * 2 + c) * 16 + 15 - k]
                block = v_buf[s, b]
                for h in range(3):
                    stv[j, h, s, pl.ds(k * BLK, BLK), :] = block[:, h * HD : (h + 1) * HD]
        return carry

    def stage_k(j, carry):
        for g in range(4):
            for k in range(2):
                b = smem_row[j, (g * 8 + yc) * 16 + 15 - k]
                block = k_buf[g, b]
                for h in range(3):
                    stk[g, h, j, pl.ds(k * BLK, BLK), :] = block[:, h * HD : (h + 1) * HD]
        return carry

    order = (4, 5, 3, 2, 6, 7, 1)
    with jax.named_scope("stage"):
        lax.fori_loop(0, 8, stage_k, 0)
        lax.fori_loop(0, 8, stage_v, 0)
    with jax.named_scope("sends"):
        send_k(0)
        each_v(lambda n: slot_v(n, 0).start())
        send_k(1)
        for unit in range(2, AHEAD):
            send_k(unit)
    for h in range(3):
        for g in range(4):
            fark[g, h, pl.ds(yc, 1)] = stk[g, h, pl.ds(yc, 1)]
        for s in range(4):
            farv[pl.ds(z, 1), h, s, pl.ds(c, 1)] = stv[pl.ds(zc, 1), h, s].reshape(1, 1, 64, HD)

    with jax.named_scope("drain1"):
        for ring in (xr, kr, vr):
            ring.drain()
        sent_bytes(req_row.at[pl.ds(0, 7)], req_send)
        sent_bytes(req_row.at[pl.ds(0, 7)], req_send)

    def hand(slot, start, size):
        view = wo_buf.at[slot, pl.ds(base + start, size)]
        pltpu.make_async_remote_copy(
            src_ref=view,
            dst_ref=view,
            send_sem=d_send,
            recv_sem=d_recv,
            device_id=(z, y, 1 - c, t),
            device_id_type=MESH,
        ).start()

    def out_sides(i):
        with jax.named_scope("osides"):
            orr.wait_sides(i)
        orr.forward(i)
        for slot in (orr.left, orr.right):
            hand(slot, *outs[i])

    out_sides(0)

    def share(h, n):
        s = lax.rem(t + n, 4)
        cols = pl.ds(h * HD, HD)
        return pltpu.make_async_remote_copy(
            src_ref=att_buf.at[pl.ds(s * 128, 128), cols],
            dst_ref=attx.at[t, :, cols],
            send_sem=a_send,
            recv_sem=a_recv.at[h // 2, n],
            device_id=(z, y, c, s),
            device_id_type=MESH,
        )

    for unit in range(12):
        h, step = divmod(unit, 4)
        with jax.named_scope("ksent"):
            wait_sent_k(unit)
        if unit + AHEAD < 12:
            send_k(unit + AHEAD)
        if unit == 1:
            each_v(lambda n: slot_v(n, 1).start())
        if unit == 5:
            each_v(lambda n: slot_v(n, 2).start())
        if unit == 3:
            out_sides(1)

        @pl.when(step <= z)
        def _():
            g = z - step
            with jax.named_scope("wk"):
                sent_bytes(fark.at[g, h, pl.ds(0, 7)], ks_recv.at[g, h])
            with jax.named_scope("wv"):
                for core in range(2):

                    @pl.when(g * 2 + core != zc)
                    def _():
                        wait_v(g * 2 + core, h)

            with jax.named_scope("far"):
                bias = bias_far[g]
                s = score(fark[g, h].reshape(512, HD), h).reshape(16, 32, 512)
                s = (s + bias[:, None, :]).reshape(512, 512)
                absorb(h, s, farv[g, h].reshape(512, HD))

        if step == 3:
            with jax.named_scope("finish"):
                attended = acc_buf[h] / l_buf[h]
                att_buf[:, h * HD : (h + 1) * HD] = attended.T.astype(BF16)
                for n in (2, 1, 3):
                    share(h, n).start()

    with jax.named_scope("oopp"):
        for i in range(2):
            orr.wait_opp(i)
            hand(orr.opp, *outs[i])

    total = dot(att_buf[pl.ds(pl.multiple_of(t * 128, 128), 128), :], wo_buf[t])
    with jax.named_scope("handed"):
        sent_bytes(wo_buf.at[pl.ds(0, 3), pl.ds(0, 192)], d_recv)
    for n in (1, 3, 2):
        s = lax.rem(t + n, 4)
        with jax.named_scope("awaited"):
            sent_bytes(attx.at[s, :, pl.ds(0, 2 * HD)], a_recv.at[0, 4 - n])
        with jax.named_scope("outn"):
            total = total + dot(attx[s, :, 0 : 2 * HD], wo_buf[s, 0 : 2 * HD, :])
    for n in (1, 3, 2):
        s = lax.rem(t + n, 4)
        with jax.named_scope("awaited2"):
            sent_bytes(attx.at[s, :, pl.ds(2 * HD, HD)], a_recv.at[1, 4 - n])
        with jax.named_scope("outn2"):
            total = total + dot(attx[s, :, 2 * HD : 3 * HD], wo_buf[s, 2 * HD : 3 * HD, :])
    out_ref[...] = total.astype(BF16)

    with jax.named_scope("drain2"):
        orr.drain()
        sent_bytes(wo_buf.at[pl.ds(0, 3), pl.ds(0, 192)], d_send)
        sent_bytes(attx.at[pl.ds(0, 3)], a_send)
        each_v(lambda n: slot_v(n, 0).wait_send())
        each_v(lambda n: slot_v(n, 1).wait_send())
        each_v(lambda n: slot_v(n, 2).wait_send())


def local(tokens, w_query, w_key, w_value, w_out, chosen):
    any_ = pl.BlockSpec(memory_space=pltpu.HBM)
    vmem = pl.BlockSpec(memory_space=pltpu.VMEM)
    dma = pltpu.SemaphoreType.DMA
    return pl.pallas_call(
        body,
        out_shape=jax.ShapeDtypeStruct((128, 2048), BF16),
        in_specs=[any_] * 5 + [vmem],
        out_specs=vmem,
        scratch_shapes=[
            pltpu.VMEM((4, 512, 512), BF16),
            pltpu.VMEM((4, 512, 1152), BF16),
            pltpu.VMEM((512, 384), BF16),
            pltpu.VMEM((4, 16, 32, 384), BF16),
            pltpu.VMEM((4, 16, 32, 384), BF16),
            pltpu.VMEM((4, 384, 2048), BF16),
            pltpu.VMEM((4, 3, 8, 64, HD), BF16),
            pltpu.VMEM((8, 3, 4, 64, HD), BF16),
            pltpu.VMEM((4, 3, 8, 64, HD), BF16),
            pltpu.VMEM((4, 3, 4, 2, 64, HD), BF16),
            pltpu.VMEM((512, 384), BF16),
            pltpu.VMEM((4, 128, 384), BF16),
            pltpu.VMEM((512, 512), F32),
            pltpu.VMEM((5, 16, 512), F32),
            pltpu.VMEM((3, 1, 512), F32),
            pltpu.VMEM((3, 1, 512), F32),
            pltpu.VMEM((3, 128, 512), F32),
            pltpu.VMEM((8, 8, 512), jnp.int32),
            pltpu.VMEM((8, 8, 512), jnp.int32),
            pltpu.SMEM((8, 512), jnp.int32),
            pltpu.SMEM((8, 512), jnp.int32),
            dma((7,)),
            dma,
            dma((2,)),
            dma, dma((4, CHUNKS)), dma, dma((4, CHUNKS)),
            dma, dma((4, CHUNKS)), dma, dma((4, 2)),
            dma((12,)), dma((4, 3)), dma((3, 8)), dma((3, 8)),
            dma, dma, dma, dma((2, 4)),
        ],
        compiler_params=pltpu.CompilerParams(
            collective_id=0, has_side_effects=True, vmem_limit_bytes=56_000_000
        ),
        name="layer",
    )(
        tokens,
        w_query.reshape(4, 512, 384),
        w_key.reshape(4, 512, 384),
        w_value.reshape(4, 512, 384),
        w_out,
        chosen,
    )


def solution(mesh):
    finer = Mesh(mesh.devices.reshape(4, 4, 2, mesh.shape["tp"]), KV_TP)
    placed = (P(KV, "tp"), P(None, "tp"), P(None, "tp"), P(None, "tp"), P("tp", None), P(KV, None))
    return jax.shard_map(
        local, mesh=finer, in_specs=placed, out_specs=P(KV_TP, None), check_vma=False
    )
```
